512 devices in a mesh: ep: 32 (over z, core), tp: 16 (over y, x).
Axes of the slice: x: 4, y: 4, z: 16, core: 2. Of those that a mesh axis runs over, the one named last changes fastest.
Arguments:
- tokens: bfloat16 [2048, 2048], P('ep', 'tp'), may hold values from -20 to 20
- state: float32 [2048, 16, 64, 64], P('ep', 'tp'), may hold values from -1.5 to 1.5
- attn_gain: float32 [2048], replicated, may hold values from 0.1 to 1.9
- ffn_gain: float32 [2048], replicated, may hold values from 0.1 to 1.9
- w_query: bfloat16 [2048, 1024], P(None, 'tp'), may hold values from -0.125 to 0.125
- w_key: bfloat16 [2048, 1024], P(None, 'tp'), may hold values from -0.125 to 0.125
- w_value: bfloat16 [2048, 1024], P(None, 'tp'), may hold values from -0.125 to 0.125
- w_output_gate: bfloat16 [2048, 1024], P(None, 'tp'), may hold values from -0.125 to 0.125
- w_decay: bfloat16 [2048, 16], replicated, may hold values from -0.125 to 0.125
- w_beta: bfloat16 [2048, 16], replicated, may hold values from -0.125 to 0.125
- decay_rate: float32 [16], P('tp'), may hold values from 0.1 to 2
- decay_shift: float32 [16], P('tp'), may hold values from -2 to 1
- head_gain: float32 [64], replicated, may hold values from 0.1 to 1.9
- w_mix_out: bfloat16 [1024, 2048], P(None, 'tp'), may hold values from -0.1875 to 0.1875
- expert_ids: int32 [2048, 2], P('ep'), may hold values from 0 to 31, all different within a row; in each aligned block of 64 rows (0 to 63, 64 to 127, ...) at most 8 rows name the same one
- expert_weights: float32 [2048, 2], P('ep'), may hold values from 0.2 to 1
- w_gate: bfloat16 [32, 2048, 4096], P('ep', None, 'tp'), may hold values from -0.125 to 0.125
- w_up: bfloat16 [32, 2048, 4096], P('ep', None, 'tp'), may hold values from -0.125 to 0.125
- w_down: bfloat16 [32, 4096, 2048], P('ep', 'tp'), may hold values from -0.09375 to 0.09375
Outputs:
- layer_out: bfloat16 [2048, 2048], P('ep', 'tp')
- new_state: float32 [2048, 16, 64, 64], P('ep', 'tp')
The draws below stay inside these ranges and needn't reach their ends.
Inputs may be any that keep to these rules, and one draw needn't show every extreme that they name: `expert_ids`: each row names 2 different experts; within the rows of one index of ep (aligned blocks of 64 rows) no expert is named by more than 8 rows, and in some blocks one expert is named by exactly 8 rows.
All inputs are finite; a program needn't handle non-finite values.
Results may differ from the reference program's by a relative error of at most 0.013.
Values may be sent and summed in bfloat16 or wider, within the bound.
No kernel may reach another device: no remote copies, remote signals or barrier semaphores. Data moves between devices by JAX's collectives and lax.ppermute only.
A program may use at most 64 MiB of HBM per device.

```python
import math
import jax
import jax.numpy as jnp
import numpy as np
from jax import lax

D = 2048
HEADS = 16
HEAD_DIM = 64
DN_W = 1024
FF = 4096
EXPERTS = 32
TOPK = 2
SEQS = 64
TOKENS = 2048
CAP = 8
N_EP = 32
N_TP = 16


def draw_tokens(key, part):
    key_rows = jax.random.fold_in(key, 11)
    key_cols = jax.random.fold_in(key, 12)
    key_vals = jax.random.fold_in(key, 13)
    row_scale = jnp.exp(jax.random.uniform(key_rows, (TOKENS, 1), jnp.float32, math.log(0.5), math.log(2.0)))
    rising = jnp.exp(jnp.linspace(math.log(0.5), math.log(1.5), D, dtype=jnp.float32))
    rough = jnp.exp(jax.random.uniform(key_cols, (D,), jnp.float32, math.log(0.8), math.log(1.25)))
    col_scale = (rising * rough)[None, :]
    values = jnp.clip(jax.random.normal(key_vals, (TOKENS, D), jnp.float32), -4.0, 4.0)
    return (values * row_scale * col_scale).astype(jnp.bfloat16)


def steps_of(key, shape, cuts, least, top_value):
    factor_of = 1.0
    for axis_at, shards_of in cuts:
        draws = jax.random.uniform(jax.random.fold_in(jax.random.fold_in(key, 6), axis_at), (shards_of,), jnp.float32, least / len(cuts), top_value / len(cuts))
        factor_of = factor_of * jnp.repeat(jnp.exp(draws), shape[axis_at] // shards_of).reshape((-1,) + (1,) * (len(shape) - 1 - axis_at))
    return factor_of


def shared_out(own_key, own, number, rows, number_of, top, reach, slope):
    ranking = jax.random.permutation(own_key, number_of)
    crowded, usual = portions_of(number_of, rows * top, reach, slope, True), portions_of(number_of, rows * top, reach, slope, False)
    places = jnp.arange(number_of)

    def named(lengths, turn):
        used = int((lengths > 0).sum())
        fixed = max(1, used // 4)
        moved = fixed + (places - fixed + turn * (used - fixed)) % max(1, number_of - fixed)
        return jnp.zeros((number_of,), jnp.int32).at[ranking[jnp.where(places < fixed, places, moved)]].set(jnp.asarray(lengths, jnp.int32))

    lengths = jnp.where(number % 4 == 0, named(crowded, number // 4), named(usual, number - number // 4 - 1))
    mixed = jax.random.permutation(jax.random.fold_in(own, 3), number_of)
    giver, taker = mixed[0:number_of // 2 * 2:2], mixed[1:number_of // 2 * 2:2]
    room = jnp.minimum(lengths[giver] - 1, reach - lengths[taker]) // 2
    room = jnp.where((giver == ranking[0]) | (taker == ranking[0]) | (lengths[taker] == 0), 0, jnp.maximum(room, 0))
    moved = jax.random.randint(jax.random.fold_in(own, 4), (number_of // 2,), 0, 1 << 20) % (room + 1)
    lengths = lengths.at[giver].add(-moved).at[taker].add(moved)
    items = jnp.searchsorted(jnp.cumsum(lengths), jnp.arange(rows * top), side="right").astype(jnp.int32)
    grid = items.reshape(top, rows).T
    grid = grid[jax.random.permutation(jax.random.fold_in(own, 1), rows)]
    turn = jax.random.randint(jax.random.fold_in(own, 2), (rows, 1), 0, top)
    return jnp.take_along_axis(grid, (jnp.arange(top)[None, :] + turn) % top, axis=1)


def portions_of(amount, total, reach, skew, full):
    portions = [(1 << 20) // math.isqrt(grade ** skew) + 1 for grade in range(1, amount + 1)]
    largest = reach if full else min(reach, max(-(-total // amount), total * portions[0] // sum(portions)))
    least = 1 if total - largest >= amount - 1 else 0
    given, surplus = [largest] + [least] * (amount - 1), total - largest - least * (amount - 1)
    while surplus > 0:
        free = [i for i in range(1, amount) if given[i] < largest] or [i for i in range(1, amount) if given[i] < reach]
        mass, left = sum([portions[i] for i in free]), surplus
        for i in free:
            addition = min(reach - given[i], max(1, left * portions[i] // mass), surplus)
            given[i] = given[i] + addition
            surplus = surplus - addition
    return np.array(given)


def centred(key, dims, spread, most, split=(), kind=jnp.bfloat16):
    loudness = steps_of(key, dims, split, -0.22, 0.18) if split else 1.0
    values = jax.random.normal(key, dims, jnp.float32) * spread * loudness
    return jnp.minimum(jnp.maximum(values, -most), most).astype(kind)


def setup_inputs(seed: int = 0) -> dict:
    arg_keys = jax.random.split(jax.random.key(seed), 20)
    tokens = draw_tokens(jax.random.fold_in(arg_keys[19], 71), 0)
    state = centred(arg_keys[1], (TOKENS, HEADS, HEAD_DIM, HEAD_DIM), 0.3, 1.5, ((0, 32), (1, 16)), jnp.float32)
    attn_gain = jnp.clip(1.0 + 0.18 * jax.random.normal(arg_keys[2], (D,), jnp.float32), 0.1, 1.9)
    ffn_gain = jnp.clip(1.0 + 0.18 * jax.random.normal(arg_keys[3], (D,), jnp.float32), 0.1, 1.9)
    w_query = centred(arg_keys[4], (D, DN_W), D ** -0.5, 0.125, ((1, 16),))
    w_key = centred(arg_keys[5], (D, DN_W), D ** -0.5, 0.125, ((1, 16),))
    w_value = centred(arg_keys[6], (D, DN_W), D ** -0.5, 0.125, ((1, 16),))
    w_output_gate = centred(arg_keys[7], (D, DN_W), D ** -0.5, 0.125, ((1, 16),))
    w_decay = centred(arg_keys[8], (D, HEADS), D ** -0.5, 0.125)
    w_beta = centred(arg_keys[9], (D, HEADS), D ** -0.5, 0.125)
    decay_rate = jnp.clip(jnp.exp(math.log(2.0) - 2.9957323 * jax.random.uniform(arg_keys[10], (HEADS,), jnp.float32) ** steps_of(arg_keys[10], (HEADS,), ((0, 16),), -0.2, 0.2)), 0.1, 2.0)
    decay_shift = jnp.clip(-2.0 + 3.0 * jax.random.uniform(arg_keys[11], (HEADS,), jnp.float32) ** steps_of(arg_keys[11], (HEADS,), ((0, 16),), -0.2, 0.2), -2.0, 1.0)
    head_gain = jnp.clip(1.0 + 0.18 * jax.random.normal(arg_keys[12], (HEAD_DIM,), jnp.float32), 0.1, 1.9)
    w_mix_out = centred(arg_keys[13], (DN_W, D), DN_W ** -0.5, 0.1875, ((1, 16),))
    expert_ids_keys = jax.random.split(jax.random.fold_in(arg_keys[14], 1), TOKENS // SEQS)
    expert_ids_turns = jax.random.permutation(jax.random.fold_in(arg_keys[14], 3), TOKENS // SEQS)
    expert_ids = jax.vmap(lambda own, number: shared_out(jax.random.fold_in(arg_keys[14], 2), own, number, SEQS, EXPERTS, TOPK, CAP, 1))(expert_ids_keys, expert_ids_turns).reshape((TOKENS, TOPK))
    expert_weights = jnp.clip(0.2 + 0.8 * jax.random.uniform(arg_keys[15], (TOKENS, TOPK), jnp.float32) ** steps_of(arg_keys[15], (TOKENS, TOPK), ((0, 32),), -0.2, 0.2), 0.2, 1.0)
    w_gate = centred(arg_keys[16], (EXPERTS, D, FF), D ** -0.5, 0.125, ((0, 32), (2, 16)))
    w_up = centred(arg_keys[17], (EXPERTS, D, FF), D ** -0.5, 0.125, ((0, 32), (2, 16)))
    w_down = centred(arg_keys[18], (EXPERTS, FF, D), FF ** -0.5, 0.09375, ((0, 32), (1, 16)))
    return dict(tokens=tokens, state=state, attn_gain=attn_gain, ffn_gain=ffn_gain, w_query=w_query, w_key=w_key, w_value=w_value, w_output_gate=w_output_gate, w_decay=w_decay, w_beta=w_beta, decay_rate=decay_rate, decay_shift=decay_shift, head_gain=head_gain, w_mix_out=w_mix_out, expert_ids=expert_ids, expert_weights=expert_weights, w_gate=w_gate, w_up=w_up, w_down=w_down)


EPS = 1e-06

def rms_scale(values):
    return lax.rsqrt(lax.optimization_barrier(jnp.mean(values * values, axis=-1, keepdims=True)) + EPS)

def unit_norm(values):
    return values * lax.rsqrt(lax.optimization_barrier(jnp.sum(values * values, axis=-1, keepdims=True)) + EPS)

def stored(values):
    return lax.optimization_barrier(values.astype(jnp.bfloat16)).astype(jnp.float32)

def slot_tables(expert_ids, expert_weights):
    pair_count = SEQS * TOPK
    block_ids = expert_ids.reshape(N_EP, pair_count)
    one_hot = (block_ids[:, :, None] == jnp.arange(EXPERTS, dtype=jnp.int32)[None, None, :]).astype(jnp.int32)
    earlier = jnp.cumsum(one_hot, axis=1) - one_hot
    slot_rank = lax.optimization_barrier(jnp.sum(earlier * one_hot, axis=2)).astype(jnp.int32)
    block_index = jnp.arange(N_EP, dtype=jnp.int32)[:, None]
    position = (block_ids * (N_EP * CAP) + block_index * CAP + slot_rank).reshape(-1)
    token_of = (jnp.arange(TOKENS * TOPK, dtype=jnp.int32) // TOPK).astype(jnp.int32)
    table_token = jnp.zeros((EXPERTS * N_EP * CAP,), jnp.int32).at[position].set(token_of)
    table_weight = jnp.zeros((EXPERTS * N_EP * CAP,), jnp.float32).at[position].set(expert_weights.reshape(-1))
    return (table_token, table_weight)

def reference(tokens, state, attn_gain, ffn_gain, w_query, w_key, w_value, w_output_gate, w_decay, w_beta, decay_rate, decay_shift, head_gain, w_mix_out, expert_ids, expert_weights, w_gate, w_up, w_down):
    tokens_f32 = tokens.astype(jnp.float32)
    normed = (tokens_f32 * rms_scale(tokens_f32) * attn_gain).astype(jnp.bfloat16)

    def project(weight):
        return jnp.dot(normed, weight, preferred_element_type=jnp.float32)

    def by_head(values):
        return values.reshape(TOKENS, HEADS, HEAD_DIM)
    query_proj = stored(project(w_query))
    key_proj = stored(project(w_key))
    value_proj = stored(project(w_value))
    gate_proj = stored(project(w_output_gate))
    keep_rate = jnp.exp(-decay_rate * jax.nn.softplus(project(w_decay) + decay_shift))
    beta_gate = jax.nn.sigmoid(project(w_beta))
    query_head = unit_norm(jax.nn.silu(by_head(query_proj))) * HEAD_DIM ** (-0.5)
    key_head = unit_norm(jax.nn.silu(by_head(key_proj)))
    value_head = jax.nn.silu(by_head(value_proj))
    decayed = keep_rate[:, :, None, None] * state
    recalled = jnp.einsum('thd,thde->the', key_head, decayed, precision=lax.Precision.HIGHEST)
    correction = beta_gate[:, :, None] * (value_head - recalled)
    new_state = decayed + key_head[:, :, :, None] * correction[:, :, None, :]
    reading = jnp.einsum('thd,thde->the', query_head, new_state, precision=lax.Precision.HIGHEST)
    head_out = (reading * rms_scale(reading) * head_gain * jax.nn.silu(by_head(gate_proj))).astype(jnp.bfloat16)
    mixed = jnp.dot(head_out.reshape(TOKENS, DN_W), w_mix_out, preferred_element_type=jnp.float32)
    residual = (tokens_f32 + mixed).astype(jnp.bfloat16)
    residual_f32 = residual.astype(jnp.float32)
    normed_ffn = (residual_f32 * rms_scale(residual_f32) * ffn_gain).astype(jnp.bfloat16)
    table_token, table_weight = slot_tables(expert_ids, expert_weights)

    def one_expert(operands):
        token_list, gate_weight, up_weight, down_weight = operands
        inputs = normed_ffn[token_list]
        gate_sum = jnp.dot(inputs, gate_weight, preferred_element_type=jnp.float32)
        up_sum = jnp.dot(inputs, up_weight, preferred_element_type=jnp.float32)
        expert_hidden = (jax.nn.silu(gate_sum) * up_sum).astype(jnp.bfloat16)
        split_hidden = expert_hidden.reshape(N_EP * CAP, N_TP, FF // N_TP).astype(jnp.float32)
        split_down = down_weight.reshape(N_TP, FF // N_TP, D).astype(jnp.float32)
        partial_value = jnp.einsum('rjf,jfd->jrd', split_hidden, split_down).astype(jnp.bfloat16)
        return lax.optimization_barrier(jnp.sum(partial_value.astype(jnp.float32), axis=0)).astype(jnp.bfloat16)
    expert_out = lax.map(one_expert, (table_token.reshape(EXPERTS, N_EP * CAP), w_gate, w_up, w_down))
    weighted = table_weight[:, None] * expert_out.reshape(EXPERTS * N_EP * CAP, D).astype(jnp.float32)
    routed = jnp.zeros((TOKENS, D), jnp.float32).at[table_token].add(weighted)
    layer_out = (residual_f32 + routed).astype(jnp.bfloat16)
    return (layer_out, new_state)
```

```python
import jax
import jax.numpy as jnp
from jax import lax
from jax.sharding import Mesh, PartitionSpec as P

EPS = 1e-06
TP = ("y", "x")
PLANE = ("c", "y", "x")


def exchanged(blocks, axes):
    return lax.all_to_all(blocks, axes, 0, 0, tiled=True)


def to_everyone(shard, axes):
    count = lax.axis_size(axes)
    return exchanged(jnp.broadcast_to(shard[None], (count, *shard.shape)), axes)


def unit_norm(values):
    return values * lax.rsqrt(jnp.sum(values * values, axis=-1, keepdims=True) + EPS)


def stored(values):
    return lax.optimization_barrier(values.astype(jnp.bfloat16)).astype(jnp.float32)


def row_norm(values, gain):
    scale = lax.rsqrt(jnp.mean(values * values, axis=1, keepdims=True) + EPS)
    return (values * scale * gain).astype(jnp.bfloat16)


def side_by_side(blocks):
    return jnp.moveaxis(blocks, 0, 1).reshape(blocks.shape[1], -1)


def shards(
    tokens,
    state,
    attn_gain,
    ffn_gain,
    w_query,
    w_key,
    w_value,
    w_output_gate,
    w_decay,
    w_beta,
    decay_rate,
    decay_shift,
    head_gain,
    w_mix_out,
    expert_ids,
    expert_weights,
    w_gate,
    w_up,
    w_down,
):
    planes = lax.axis_size("z")
    cores = lax.axis_size("c")
    tp_size = lax.axis_size(TP)
    seq_count = tokens.shape[0]
    own_width = tokens.shape[1]
    head_dim = head_gain.shape[0]
    top_count = expert_ids.shape[1]
    expert_total = planes * cores
    capacity = 2 * seq_count * top_count // expert_total

    experts = jnp.arange(expert_total, dtype=jnp.int32)
    one_hot = (expert_ids[:, :, None] == experts).astype(jnp.float32)
    position = jnp.arange(seq_count, dtype=jnp.int32)
    before = (position[:, None] > position[None, :]).astype(jnp.float32)
    earlier = jnp.dot(before, jnp.sum(one_hot, axis=1))
    slots = jnp.arange(expert_total * capacity, dtype=jnp.int32)
    hits = []
    for choice in range(top_count):
        rank = jnp.sum(earlier * one_hot[:, choice], axis=1).astype(jnp.int32)
        slot = expert_ids[:, choice] * capacity + rank
        hits.append(slot[:, None] == slots[None, :])
    pick = (hits[0] | hits[1]).astype(jnp.bfloat16)
    hits = [hit.astype(jnp.bfloat16) for hit in hits]

    whole = side_by_side(to_everyone(tokens, TP)).astype(jnp.float32)
    normed = row_norm(whole, attn_gain)

    def project(weight):
        return jnp.dot(normed, weight, preferred_element_type=jnp.float32)

    head = lax.axis_index(TP)
    decay_col = lax.dynamic_slice_in_dim(w_decay, head, 1, 1)
    beta_col = lax.dynamic_slice_in_dim(w_beta, head, 1, 1)
    query_proj = stored(project(w_query))
    key_proj = stored(project(w_key))
    value_proj = stored(project(w_value))
    gate_proj = stored(project(w_output_gate))
    keep_rate = jnp.exp(-decay_rate * jax.nn.softplus(project(decay_col) + decay_shift))
    beta_gate = jax.nn.sigmoid(project(beta_col))
    query_head = unit_norm(jax.nn.silu(query_proj)) * head_dim ** (-0.5)
    key_head = unit_norm(jax.nn.silu(key_proj))
    value_head = jax.nn.silu(value_proj)
    decayed = keep_rate[:, :, None] * state[:, 0]
    recalled = jnp.einsum("td,tde->te", key_head, decayed, precision=lax.Precision.HIGHEST)
    correction = beta_gate * (value_head - recalled)
    new_state = decayed + key_head[:, :, None] * correction[:, None, :]
    reading = jnp.einsum("td,tde->te", query_head, new_state, precision=lax.Precision.HIGHEST)
    reading_scale = lax.rsqrt(jnp.mean(reading * reading, axis=-1, keepdims=True) + EPS)
    head_out = (reading * reading_scale * head_gain * jax.nn.silu(gate_proj)).astype(jnp.bfloat16)

    all_heads = side_by_side(to_everyone(head_out, TP))
    mixed = jnp.dot(all_heads, w_mix_out, preferred_element_type=jnp.float32)
    residual = (tokens.astype(jnp.float32) + mixed).astype(jnp.bfloat16)

    outgoing = lax.dot_general(
        pick, residual, (((0,), (0,)), ((), ())), preferred_element_type=jnp.float32
    ).astype(jnp.bfloat16)
    along_z = exchanged(outgoing.reshape(planes, cores * capacity, own_width), "z")
    per_core = jnp.moveaxis(along_z.reshape(planes, cores, capacity, own_width), 1, 0)
    half_rows = planes * capacity
    spread = jnp.broadcast_to(
        per_core.reshape(cores, 1, half_rows, own_width), (cores, tp_size, half_rows, own_width)
    )
    arrived = exchanged(spread.reshape(cores * tp_size, half_rows, own_width), PLANE)
    arrived = arrived.reshape(cores, tp_size, half_rows, own_width)
    rows = jnp.moveaxis(arrived, 1, 2).reshape(cores * half_rows, tp_size * own_width)
    rows = row_norm(rows.astype(jnp.float32), ffn_gain)

    gate_part = jnp.dot(rows, w_gate[0], preferred_element_type=jnp.float32)
    up_part = jnp.dot(rows, w_up[0], preferred_element_type=jnp.float32)
    hidden = (jax.nn.silu(gate_part) * up_part).astype(jnp.bfloat16)
    partial_value = jnp.dot(hidden, w_down[0], preferred_element_type=jnp.float32)
    partial_value = partial_value.astype(jnp.bfloat16)
    parts = jnp.moveaxis(partial_value.reshape(cores, half_rows, tp_size, own_width), 2, 1)
    parts = exchanged(parts.reshape(cores * tp_size, half_rows, own_width), PLANE)
    parts = parts.reshape(cores, tp_size, half_rows, own_width).astype(jnp.float32)
    summed = jnp.sum(parts, axis=1).astype(jnp.bfloat16)
    back = jnp.moveaxis(summed.reshape(cores, planes, capacity, own_width), 0, 1)
    returned = exchanged(back.reshape(planes, cores * capacity, own_width), "z")
    returned = returned.reshape(expert_total * capacity, own_width)

    weighted = 0.0
    for choice in range(top_count):
        pair = jnp.dot(hits[choice], returned, preferred_element_type=jnp.float32)
        weighted += pair * expert_weights[:, choice : choice + 1]
    layer_out = (residual.astype(jnp.float32) + weighted).astype(jnp.bfloat16)
    return (layer_out, new_state[:, None])


def solution(mesh):
    axes = Mesh(mesh.devices.reshape(16, 2, 4, 4), ("z", "c", "y", "x"))
    ep = ("z", "c")
    in_specs = (
        P(ep, TP),
        P(ep, TP, None, None),
        P(),
        P(),
        P(None, TP),
        P(None, TP),
        P(None, TP),
        P(None, TP),
        P(),
        P(),
        P(TP),
        P(TP),
        P(),
        P(None, TP),
        P(ep, None),
        P(ep, None),
        P(ep, None, TP),
        P(ep, None, TP),
        P(ep, TP, None),
    )
    out_specs = (P(ep, TP), P(ep, TP, None, None))
    return jax.shard_map(shards, mesh=axes, in_specs=in_specs, out_specs=out_specs, check_vma=False)
```

```python
import functools

import jax
import jax.numpy as jnp
from jax import lax
from jax.experimental import pallas as pl
from jax.experimental.pallas import tpu as pltpu
from jax.sharding import Mesh, PartitionSpec as P

EPS = 1e-06
TP = ("y", "x")
PLANE = ("c", "y", "x")
BF16 = jnp.bfloat16
F32 = jnp.float32
VMEM_LIMIT = 12 << 20


def exchanged(blocks, axes):
    return lax.all_to_all(blocks, axes, 0, 0, tiled=True)


def to_everyone(shard, axes):
    count = lax.axis_size(axes)
    return exchanged(jnp.broadcast_to(shard[None], (count, *shard.shape)), axes)


def silu(values):
    return values * (1.0 / (1.0 + jnp.exp(-values)))


def rounded(values):
    return values.astype(BF16).astype(F32)


def local_call(kernel, out_shapes, scratch, flops, *operands, scalars=()):
    vmem = pl.BlockSpec(memory_space=pltpu.VMEM)
    smem = pl.BlockSpec(memory_space=pltpu.SMEM)
    outs = [jax.ShapeDtypeStruct(shape, dtype) for shape, dtype in out_shapes]
    return pl.pallas_call(
        kernel,
        out_shape=outs,
        in_specs=[vmem] * len(operands) + [smem] * len(scalars),
        out_specs=[vmem] * len(outs),
        scratch_shapes=scratch,
        compiler_params=pltpu.CompilerParams(vmem_limit_bytes=VMEM_LIMIT),
        cost_estimate=pl.CostEstimate(flops=flops, bytes_accessed=1 << 20, transcendentals=0),
    )(*operands, *scalars)


def prepare_kernel(expert_total, capacity, ids, w_decay, w_beta, head, w_rates, slots):
    model_width = w_rates.shape[1]
    rows = []
    for weight in (w_decay, w_beta):
        values = weight[...].astype(F32)
        own = lax.broadcasted_iota(jnp.int32, values.shape, 0) == head[0]
        rows.append(jnp.sum(jnp.where(own, values, 0.0), axis=0, keepdims=True))
    row = lax.broadcasted_iota(jnp.int32, w_rates.shape, 0)
    w_rates[...] = jnp.where(row == 0, rows[0], jnp.where(row == 1, rows[1], 0.0)).astype(BF16)
    choices, seqs = ids.shape
    experts = lax.broadcasted_iota(jnp.int32, (expert_total, seqs), 0)
    chosen = [(ids[choice : choice + 1, :] == experts).astype(F32) for choice in range(choices)]
    source = lax.broadcasted_iota(jnp.int32, (seqs, seqs), 0)
    target = lax.broadcasted_iota(jnp.int32, (seqs, seqs), 1)
    before = (source < target).astype(F32).astype(BF16)
    earlier = jnp.dot((chosen[0] + chosen[1]).astype(BF16), before, preferred_element_type=F32)
    for choice in range(choices):
        rank = jnp.sum(earlier * chosen[choice], axis=0, keepdims=True).astype(jnp.int32)
        slots[choice : choice + 1, :] = ids[choice : choice + 1, :] * capacity + rank


def slot_hits(slots, slot_count):
    places = lax.broadcasted_iota(jnp.int32, (slot_count, slots.shape[1]), 0)
    return [(slots[choice : choice + 1, :] == places).astype(F32).astype(BF16) for choice in range(2)]


def lane_pair(left, right):
    shape = (left.shape[0], 128)
    lane = lax.broadcasted_iota(jnp.int32, shape, 1)
    return jnp.where(lane < 64, jnp.broadcast_to(left, shape), jnp.broadcast_to(right, shape))


def attend_kernel(tok, gain, wq, wk, wv, wg, w_rates, head_gain, state, rate, shift,
                  spread, corr_out, keep_out, key_out, normed, from_key, from_query):
    tiles, seqs, width = tok.shape
    head_dim = wq.shape[0]
    half = seqs // 2
    squares = jnp.zeros((seqs, width), F32)
    for tile in range(tiles):
        x = tok[tile].astype(F32)
        squares += x * x
    mean = jnp.sum(squares, axis=1, keepdims=True) / (tiles * width)
    scale = lax.rsqrt(mean + EPS)
    for tile in range(tiles):
        cols = slice(tile * width, (tile + 1) * width)
        normed[:, cols] = (tok[tile].astype(F32) * scale * gain[:, cols]).astype(BF16)
    rows = normed[...]
    dims = (((1,), (1,)), ((), ()))

    def project(weight):
        return lax.dot_general(rows, weight, dims, preferred_element_type=F32)

    def project_across(weight):
        return lax.dot_general(weight, rows, dims, preferred_element_type=F32)

    def unit(values, axis):
        return values * lax.rsqrt(jnp.sum(values * values, axis=axis, keepdims=True) + EPS)

    def packed(values):
        return jnp.concatenate([values[:half], values[half:]], axis=1)

    key_across = unit(silu(rounded(project_across(wk[...]))), 0)
    query_across = unit(silu(rounded(project_across(wq[...]))), 0) * head_dim ** (-0.5)
    for t in range(half):
        u = half + t
        block = jnp.concatenate([state[t], state[u]], axis=1)
        key_pair = lane_pair(key_across[:, t : t + 1], key_across[:, u : u + 1])
        query_pair = lane_pair(query_across[:, t : t + 1], query_across[:, u : u + 1])
        from_key[t : t + 1, :] = jnp.sum(key_pair * block, axis=0, keepdims=True)
        from_query[t : t + 1, :] = jnp.sum(query_pair * block, axis=0, keepdims=True)
    key = unit(silu(rounded(project(wk[...]))), 1)
    query = unit(silu(rounded(project(wq[...]))), 1) * head_dim ** (-0.5)
    overlap = jnp.sum(query * key, axis=1, keepdims=True)
    overlap = lane_pair(overlap[:half], overlap[half:])
    value = packed(silu(rounded(project(wv[...]))))
    gate = packed(silu(rounded(project(wg[...]))))
    rates = project(w_rates[...])
    decay_in = lane_pair(rates[:half, 0:1], rates[half:, 0:1]) + shift[0]
    soft = jnp.maximum(decay_in, 0.0) + jnp.log1p(jnp.exp(-jnp.abs(decay_in)))
    keep = jnp.exp(-rate[0] * soft)
    beta = 1.0 / (1.0 + jnp.exp(-lane_pair(rates[:half, 1:2], rates[half:, 1:2])))
    corr = beta * (value - keep * from_key[...])
    reading = keep * from_query[...] + overlap * corr
    squared = reading * reading
    left = lax.broadcasted_iota(jnp.int32, squared.shape, 1) < head_dim
    means = [
        jnp.sum(jnp.where(side, squared, 0.0), axis=1, keepdims=True) / head_dim
        for side in (left, jnp.logical_not(left))
    ]
    reading_scale = lane_pair(lax.rsqrt(means[0] + EPS), lax.rsqrt(means[1] + EPS))
    gain_pair = jnp.concatenate([head_gain[...], head_gain[...]], axis=1)
    head_out = (reading * reading_scale * gain_pair * gate).astype(BF16)
    for tile in range(tiles):
        spread[tile] = head_out
    corr_out[...] = corr
    keep_out[...] = keep
    key_out[...] = key_across


def state_kernel(state, corr, keep, key_across, new_state):
    half = state.shape[0] // 2
    head_dim = key_across.shape[0]
    across = key_across[...]
    for t in range(half):
        u = half + t
        key_pair = lane_pair(across[:, t : t + 1], across[:, u : u + 1])
        block = jnp.concatenate([state[t], state[u]], axis=1)
        updated = keep[t : t + 1, :] * block + key_pair * corr[t : t + 1, :]
        new_state[t] = updated[:, :head_dim]
        new_state[u] = updated[:, head_dim:]


def mix_kernel(heads, w_mix, tokens, slots, residual, outgoing):
    tiles, half, width = heads.shape
    top, bottom = [], []
    for pair in range(tiles // 2):
        even, odd = heads[2 * pair].astype(F32), heads[2 * pair + 1].astype(F32)
        left = lax.broadcasted_iota(jnp.int32, even.shape, 1) < width // 2
        top.append(jnp.where(left, even, pltpu.roll(odd, width // 2, 1)))
        bottom.append(jnp.where(left, pltpu.roll(even, width // 2, 1), odd))
    rows = [jnp.concatenate(part, axis=1).astype(BF16) for part in (top, bottom)]
    mixed = jnp.dot(jnp.concatenate(rows, axis=0), w_mix[...], preferred_element_type=F32)
    own = (tokens[...].astype(F32) + mixed).astype(BF16)
    residual[...] = own
    first, second = slot_hits(slots, outgoing.shape[0])
    outgoing[...] = jnp.dot(first + second, own, preferred_element_type=F32).astype(BF16)


def spread_kernel(along_z, spread):
    planes = along_z.shape[0]
    cores, tiles, count, width = spread.shape
    capacity = count // planes
    rows = [along_z[plane].astype(F32) for plane in range(planes)]
    for core in range(cores):
        own = [row[core * capacity : (core + 1) * capacity] for row in rows]
        block = jnp.concatenate(own, axis=0).astype(BF16)
        for tile in range(tiles):
            spread[core, tile] = block


def expert_kernel(arrived, gain, w_gate, w_up, w_down, parts, normed):
    cores, tiles, count, width = arrived.shape
    for core in range(cores):
        squares = jnp.zeros((count, width), F32)
        for tile in range(tiles):
            x = arrived[core, tile].astype(F32)
            squares += x * x
        mean = jnp.sum(squares, axis=1, keepdims=True) / (tiles * width)
        scale = lax.rsqrt(mean + EPS)
        for tile in range(tiles):
            cols = slice(tile * width, (tile + 1) * width)
            x = arrived[core, tile].astype(F32) * scale * gain[:, cols]
            normed[core * count : (core + 1) * count, cols] = x.astype(BF16)
    rows = normed[...]
    gate = jnp.dot(rows, w_gate[...], preferred_element_type=F32)
    up = jnp.dot(rows, w_up[...], preferred_element_type=F32)
    hidden = (silu(gate) * up).astype(BF16)
    for pair in range(tiles // 2):
        cols = slice(2 * pair * width, 2 * (pair + 1) * width)
        part = jnp.dot(hidden, w_down[:, cols], preferred_element_type=F32).astype(BF16)
        for core in range(cores):
            own = part[core * count : (core + 1) * count]
            parts[core, 2 * pair] = own[:, :width]
            parts[core, 2 * pair + 1] = own[:, width:]


def total_kernel(planes, parts, back):
    cores, tiles, count, width = parts.shape
    capacity = count // planes
    sums = []
    for core in range(cores):
        total = parts[core, 0].astype(F32)
        for tile in range(1, tiles):
            total += parts[core, tile].astype(F32)
        sums.append(total)
    for plane in range(planes):
        own = [total[plane * capacity : (plane + 1) * capacity] for total in sums]
        back[plane] = jnp.concatenate(own, axis=0).astype(BF16)


def combine_kernel(returned, slots, weights, residual, layer_out):
    rows = returned[...]
    seqs = slots.shape[1]
    source = lax.broadcasted_iota(jnp.int32, (seqs, seqs), 0)
    target = lax.broadcasted_iota(jnp.int32, (seqs, seqs), 1)
    dims = (((0,), (0,)), ((), ()))
    weighted = residual[...].astype(F32)
    for choice, hit in enumerate(slot_hits(slots, rows.shape[0])):
        across = jnp.where(source == target, weights[choice : choice + 1, :], 0.0)
        weight = jnp.sum(across, axis=1, keepdims=True)
        weighted += lax.dot_general(hit, rows, dims, preferred_element_type=F32) * weight
    layer_out[...] = weighted.astype(BF16)


def shards(
    tokens,
    state,
    attn_gain,
    ffn_gain,
    w_query,
    w_key,
    w_value,
    w_output_gate,
    w_decay,
    w_beta,
    decay_rate,
    decay_shift,
    head_gain,
    w_mix_out,
    expert_ids,
    expert_weights,
    w_gate,
    w_up,
    w_down,
):
    planes = lax.axis_size("z")
    cores = lax.axis_size("c")
    tp_size = lax.axis_size(TP)
    seqs, width = tokens.shape
    head_dim = head_gain.shape[0]
    model_width = attn_gain.shape[0]
    top_count = expert_ids.shape[1]
    expert_total = planes * cores
    capacity = 2 * seqs * top_count // expert_total
    half = seqs // 2
    count = planes * capacity

    gathered = to_everyone(tokens, TP)

    slot_count = expert_total * capacity
    wide = (seqs, width)
    w_rates, slots = local_call(
        functools.partial(prepare_kernel, expert_total, capacity),
        [((8, model_width), BF16), ((top_count, seqs), jnp.int32)],
        [],
        1 << 35,
        expert_ids.T,
        w_decay.T,
        w_beta.T,
        scalars=(lax.axis_index(TP)[None],),
    )
    square = (half, 2 * head_dim)
    spread, corr, keep, key_across = local_call(
        attend_kernel,
        [((tp_size, *square), BF16), (square, F32), (square, F32), ((head_dim, seqs), F32)],
        [pltpu.VMEM((seqs, model_width), BF16), pltpu.VMEM(square, F32), pltpu.VMEM(square, F32)],
        1 << 30,
        gathered,
        attn_gain[None],
        w_query.T,
        w_key.T,
        w_value.T,
        w_output_gate.T,
        w_rates,
        head_gain[None],
        state[:, 0],
        scalars=(decay_rate, decay_shift),
    )
    heads = exchanged(spread, TP)
    (new_state,) = local_call(
        state_kernel, [((seqs, head_dim, head_dim), F32)], [], 1 << 30, state[:, 0], corr, keep, key_across
    )
    residual, outgoing = local_call(
        mix_kernel, [(wide, BF16), ((slot_count, width), BF16)], [], 1 << 28, heads, w_mix_out, tokens, slots
    )
    along_z = exchanged(outgoing.reshape(planes, cores * capacity, width), "z")
    (spread_rows,) = local_call(
        spread_kernel, [((cores, tp_size, count, width), BF16)], [], 1 << 28, along_z
    )
    arrived = exchanged(spread_rows.reshape(cores * tp_size, count, width), PLANE)
    (parts,) = local_call(
        expert_kernel,
        [((cores, tp_size, count, width), BF16)],
        [pltpu.VMEM((cores * count, model_width), BF16)],
        1 << 30,
        arrived.reshape(cores, tp_size, count, width),
        ffn_gain[None],
        w_gate[0],
        w_up[0],
        w_down[0],
    )
    parts = exchanged(parts.reshape(cores * tp_size, count, width), PLANE)
    (back,) = local_call(
        functools.partial(total_kernel, planes),
        [((planes, cores * capacity, width), BF16)],
        [],
        1 << 28,
        parts.reshape(cores, tp_size, count, width),
    )
    returned = exchanged(back, "z").reshape(expert_total * capacity, width)
    (layer_out,) = local_call(
        combine_kernel, [(wide, BF16)], [], 1 << 26, returned, slots, expert_weights.T, residual
    )
    return (layer_out, new_state[:, None])


def solution(mesh):
    axes = Mesh(mesh.devices.reshape(16, 2, 4, 4), ("z", "c", "y", "x"))
    ep = ("z", "c")
    in_specs = (
        P(ep, TP),
        P(ep, TP, None, None),
        P(),
        P(),
        P(None, TP),
        P(None, TP),
        P(None, TP),
        P(None, TP),
        P(),
        P(),
        P(TP),
        P(TP),
        P(),
        P(None, TP),
        P(ep, None),
        P(ep, None),
        P(ep, None, TP),
        P(ep, None, TP),
        P(ep, TP, None),
    )
    out_specs = (P(ep, TP), P(ep, TP, None, None))
    return jax.shard_map(shards, mesh=axes, in_specs=in_specs, out_specs=out_specs, check_vma=False)
```

```python
import functools

import jax
import jax.numpy as jnp
from jax import lax
from jax.experimental import pallas as pl
from jax.experimental.pallas import tpu as pltpu
from jax.sharding import Mesh, PartitionSpec as P

EPS = 1e-06
TP = ("y", "x")
PLANE = ("c", "y", "x")
BF16 = jnp.bfloat16
F32 = jnp.float32
VMEM_LIMIT = 12 << 20


def exchanged(blocks, axes):
    return lax.all_to_all(blocks, axes, 0, 0, tiled=True)


def silu(values):
    return values * (1.0 / (1.0 + jnp.exp(-values)))


def rounded(values):
    return values.astype(BF16).astype(F32)


def local_call(kernel, out_shapes, scratch, flops, *operands, far_outs=0):
    vmem = pl.BlockSpec(memory_space=pltpu.VMEM)
    outs = [jax.ShapeDtypeStruct(shape, dtype) for shape, dtype in out_shapes]
    return pl.pallas_call(
        kernel,
        out_shape=outs,
        in_specs=[vmem] * len(operands),
        out_specs=[vmem] * (len(outs) - far_outs) + [pl.BlockSpec(memory_space=pl.ANY)] * far_outs,
        scratch_shapes=scratch,
        compiler_params=pltpu.CompilerParams(vmem_limit_bytes=VMEM_LIMIT),
        cost_estimate=pl.CostEstimate(flops=flops, bytes_accessed=1 << 20, transcendentals=0),
    )(*operands)


def broadcast_kernel(shard, rate, shift, spread, rates):
    for tile in range(spread.shape[0]):
        spread[tile] = shard[...]
    row = lax.broadcasted_iota(jnp.int32, rates.shape, 0)
    rates[...] = jnp.where(row == 0, rate[...], shift[...])


def head_row(weight, head):
    values = weight[...].astype(F32)
    own = lax.broadcasted_iota(jnp.int32, values.shape, 0) == head
    return jnp.sum(jnp.where(own, values, 0.0), axis=0, keepdims=True)


def diagonal_masks(size):
    source = lax.broadcasted_iota(jnp.int32, (size, size), 0)
    target = lax.broadcasted_iota(jnp.int32, (size, size), 1)
    return source, target


def as_column(row):
    source, target = diagonal_masks(row.shape[1])
    return jnp.sum(jnp.where(source == target, row, 0.0), axis=1, keepdims=True)


def slot_rows(ids, expert_total, capacity):
    choices, seqs = ids.shape
    experts = lax.broadcasted_iota(jnp.int32, (expert_total, seqs), 0)
    chosen = [(ids[choice : choice + 1, :] == experts).astype(F32) for choice in range(choices)]
    source, target = diagonal_masks(seqs)
    before = (source < target).astype(F32).astype(BF16)
    earlier = jnp.dot((chosen[0] + chosen[1]).astype(BF16), before, preferred_element_type=F32)
    slots = []
    for choice in range(choices):
        rank = jnp.sum(earlier * chosen[choice], axis=0, keepdims=True).astype(jnp.int32)
        slots.append(ids[choice : choice + 1, :] * capacity + rank)
    return slots


def slot_hits(slots, slot_count):
    places = lax.broadcasted_iota(jnp.int32, (slot_count, slots[0].shape[1]), 0)
    return [(slot == places).astype(F32).astype(BF16) for slot in slots]


def lane_pair(left, right):
    shape = (left.shape[0], 128)
    lane = lax.broadcasted_iota(jnp.int32, shape, 1)
    return jnp.where(lane < 64, jnp.broadcast_to(left, shape), jnp.broadcast_to(right, shape))


def attend_kernel(tok, gain, wq, wk, wv, wg, w_decay, w_beta, head_gain, rates_in, state,
                  spread, new_state, normed, blocks, keys, from_key, from_query):
    tiles, seqs, width = tok.shape
    head_dim = wq.shape[0]
    half = seqs // 2
    squares = jnp.zeros((seqs, width), F32)
    for tile in range(tiles):
        x = tok[tile].astype(F32)
        squares += x * x
    mean = jnp.sum(squares, axis=1, keepdims=True) / (tiles * width)
    scale = lax.rsqrt(mean + EPS)
    for tile in range(tiles):
        cols = slice(tile * width, (tile + 1) * width)
        normed[:, cols] = (tok[tile].astype(F32) * scale * gain[:, cols]).astype(BF16)
    rows = normed[...]
    dims = (((1,), (1,)), ((), ()))

    def unit(values):
        return values * lax.rsqrt(jnp.sum(values * values, axis=0, keepdims=True) + EPS)

    across = lax.dot_general(
        jnp.concatenate([wq[...], wk[...]], axis=0), rows, dims, preferred_element_type=F32
    )
    across = silu(rounded(across))
    query = unit(across[:head_dim]) * head_dim ** (-0.5)
    key = unit(across[head_dim:])
    for t in range(half):
        u = half + t
        block = jnp.concatenate([state[t], state[u]], axis=1)
        key_pair = lane_pair(key[:, t : t + 1], key[:, u : u + 1])
        query_pair = lane_pair(query[:, t : t + 1], query[:, u : u + 1])
        blocks[t] = block
        keys[t] = key_pair
        from_key[t : t + 1, :] = jnp.sum(key_pair * block, axis=0, keepdims=True)
        from_query[t : t + 1, :] = jnp.sum(query_pair * block, axis=0, keepdims=True)
    overlap = as_column(jnp.sum(query * key, axis=0, keepdims=True))
    overlap = lane_pair(overlap[:half], overlap[half:])
    own = lax.dot_general(rows, jnp.concatenate([wv[...], wg[...]], axis=0), dims, preferred_element_type=F32)
    own = silu(rounded(own))
    upper, lower = own[:half], own[half:]
    left = lax.broadcasted_iota(jnp.int32, upper.shape, 1) < head_dim
    value = jnp.where(left, upper, pltpu.roll(lower, head_dim, 1))
    gate = jnp.where(left, pltpu.roll(upper, head_dim, 1), lower)
    head = lax.axis_index("y") * lax.axis_size("x") + lax.axis_index("x")
    place = lax.broadcasted_iota(jnp.int32, (8, tiles * width), 0)
    w_rates = jnp.where(place == 0, head_row(w_decay, head), jnp.where(place == 1, head_row(w_beta, head), 0.0))
    rates = lax.dot_general(rows, w_rates.astype(BF16), dims, preferred_element_type=F32)
    decay_in = lane_pair(rates[:half, 0:1], rates[half:, 0:1]) + rates_in[1:2, :]
    soft = jnp.maximum(decay_in, 0.0) + jnp.log1p(jnp.exp(-jnp.abs(decay_in)))
    keep = jnp.exp(-rates_in[0:1, :] * soft)
    beta = 1.0 / (1.0 + jnp.exp(-lane_pair(rates[:half, 1:2], rates[half:, 1:2])))
    corr = beta * (value - keep * from_key[...])
    reading = keep * from_query[...] + overlap * corr
    squared = reading * reading
    means = [
        jnp.sum(jnp.where(side, squared, 0.0), axis=1, keepdims=True) / head_dim
        for side in (left, jnp.logical_not(left))
    ]
    reading_scale = lane_pair(lax.rsqrt(means[0] + EPS), lax.rsqrt(means[1] + EPS))
    gain_pair = jnp.concatenate([head_gain[...], head_gain[...]], axis=1)
    head_out = (reading * reading_scale * gain_pair * gate).astype(BF16)
    for tile in range(tiles):
        spread[tile] = head_out
    for t in range(half):
        updated = keep[t : t + 1, :] * blocks[t] + keys[t] * corr[t : t + 1, :]
        new_state[t] = updated[:, :head_dim]
        new_state[half + t] = updated[:, head_dim:]


def mix_kernel(expert_total, heads, w_mix, tokens, ids, residual, outgoing, slots_out):
    tiles, half, width = heads.shape
    top, bottom = [], []
    for pair in range(tiles // 2):
        even, odd = heads[2 * pair].astype(F32), heads[2 * pair + 1].astype(F32)
        left = lax.broadcasted_iota(jnp.int32, even.shape, 1) < width // 2
        top.append(jnp.where(left, even, pltpu.roll(odd, width // 2, 1)))
        bottom.append(jnp.where(left, pltpu.roll(even, width // 2, 1), odd))
    rows = [jnp.concatenate(part, axis=1).astype(BF16) for part in (top, bottom)]
    mixed = jnp.dot(jnp.concatenate(rows, axis=0), w_mix[...], preferred_element_type=F32)
    own = (tokens[...].astype(F32) + mixed).astype(BF16)
    residual[...] = own
    slots = slot_rows(ids, expert_total, outgoing.shape[0] // expert_total)
    for choice, slot in enumerate(slots):
        slots_out[choice : choice + 1, :] = slot
    first, second = slot_hits(slots, outgoing.shape[0])
    outgoing[...] = jnp.dot(first + second, own, preferred_element_type=F32).astype(BF16)


def spread_kernel(along_z, spread):
    planes = along_z.shape[0]
    cores, tiles, count, width = spread.shape
    capacity = count // planes
    rows = [along_z[plane].astype(F32) for plane in range(planes)]
    for core in range(cores):
        own = [row[core * capacity : (core + 1) * capacity] for row in rows]
        block = jnp.concatenate(own, axis=0).astype(BF16)
        for tile in range(tiles):
            spread[core, tile] = block


def expert_kernel(arrived, gain, w_gate, w_up, w_down, state, parts, state_out, normed, sem):
    state_copy = pltpu.make_async_copy(state, state_out, sem)
    state_copy.start()
    cores, tiles, count, width = arrived.shape
    for core in range(cores):
        squares = jnp.zeros((count, width), F32)
        for tile in range(tiles):
            x = arrived[core, tile].astype(F32)
            squares += x * x
        mean = jnp.sum(squares, axis=1, keepdims=True) / (tiles * width)
        scale = lax.rsqrt(mean + EPS)
        for tile in range(tiles):
            cols = slice(tile * width, (tile + 1) * width)
            x = arrived[core, tile].astype(F32) * scale * gain[:, cols]
            normed[core * count : (core + 1) * count, cols] = x.astype(BF16)
    rows = normed[...]
    gate = jnp.dot(rows, w_gate[...], preferred_element_type=F32)
    up = jnp.dot(rows, w_up[...], preferred_element_type=F32)
    hidden = (silu(gate) * up).astype(BF16)
    for pair in range(tiles // 2):
        cols = slice(2 * pair * width, 2 * (pair + 1) * width)
        part = jnp.dot(hidden, w_down[:, cols], preferred_element_type=F32).astype(BF16)
        for core in range(cores):
            own = part[core * count : (core + 1) * count]
            parts[core, 2 * pair] = own[:, :width]
            parts[core, 2 * pair + 1] = own[:, width:]
    state_copy.wait()


def total_kernel(planes, parts, back):
    cores, tiles, count, width = parts.shape
    capacity = count // planes
    sums = []
    for core in range(cores):
        total = parts[core, 0].astype(F32)
        for tile in range(1, tiles):
            total += parts[core, tile].astype(F32)
        sums.append(total)
    for plane in range(planes):
        own = [total[plane * capacity : (plane + 1) * capacity] for total in sums]
        back[plane] = jnp.concatenate(own, axis=0).astype(BF16)


def combine_kernel(returned, slots, weights, residual, layer_out):
    rows = returned[...]
    dims = (((0,), (0,)), ((), ()))
    weighted = residual[...].astype(F32)
    owners = [slots[choice : choice + 1, :] for choice in range(slots.shape[0])]
    for choice, hit in enumerate(slot_hits(owners, rows.shape[0])):
        pair = lax.dot_general(hit, rows, dims, preferred_element_type=F32)
        weighted += pair * as_column(weights[choice : choice + 1, :])
    layer_out[...] = weighted.astype(BF16)


def shards(
    tokens,
    state,
    attn_gain,
    ffn_gain,
    w_query,
    w_key,
    w_value,
    w_output_gate,
    w_decay,
    w_beta,
    decay_rate,
    decay_shift,
    head_gain,
    w_mix_out,
    expert_ids,
    expert_weights,
    w_gate,
    w_up,
    w_down,
):
    planes = lax.axis_size("z")
    cores = lax.axis_size("c")
    tp_size = lax.axis_size(TP)
    seqs, width = tokens.shape
    head_dim = head_gain.shape[0]
    model_width = attn_gain.shape[0]
    top_count = expert_ids.shape[1]
    expert_total = planes * cores
    capacity = 2 * seqs * top_count // expert_total
    half = seqs // 2
    count = planes * capacity

    slot_count = expert_total * capacity
    wide = (seqs, width)
    token_spread, head_rates = local_call(
        broadcast_kernel,
        [((tp_size, *wide), BF16), ((2, 2 * head_dim), F32)],
        [],
        1 << 35,
        tokens,
        decay_rate[None],
        decay_shift[None],
    )
    gathered = exchanged(token_spread, TP)
    square = (half, 2 * head_dim)
    blocks = (half, head_dim, 2 * head_dim)
    spread, new_state = local_call(
        attend_kernel,
        [((tp_size, *square), BF16), ((seqs, head_dim, head_dim), F32)],
        [
            pltpu.VMEM((seqs, model_width), BF16),
            pltpu.VMEM(blocks, F32),
            pltpu.VMEM(blocks, F32),
            pltpu.VMEM(square, F32),
            pltpu.VMEM(square, F32),
        ],
        1 << 30,
        gathered,
        attn_gain[None],
        w_query.T,
        w_key.T,
        w_value.T,
        w_output_gate.T,
        w_decay.T,
        w_beta.T,
        head_gain[None],
        head_rates,
        state[:, 0],
    )
    heads = exchanged(spread, TP)
    residual, outgoing, slots = local_call(
        functools.partial(mix_kernel, expert_total),
        [(wide, BF16), ((slot_count, width), BF16), ((top_count, seqs), jnp.int32)],
        [],
        1 << 28,
        heads,
        w_mix_out,
        tokens,
        expert_ids.T,
    )
    along_z = exchanged(outgoing.reshape(planes, cores * capacity, width), "z")
    (spread_rows,) = local_call(
        spread_kernel, [((cores, tp_size, count, width), BF16)], [], 1 << 28, along_z
    )
    arrived = exchanged(spread_rows.reshape(cores * tp_size, count, width), PLANE)
    parts, state_out = local_call(
        expert_kernel,
        [((cores, tp_size, count, width), BF16), (new_state.shape, F32)],
        [pltpu.VMEM((cores * count, model_width), BF16), pltpu.SemaphoreType.DMA],
        1 << 30,
        arrived.reshape(cores, tp_size, count, width),
        ffn_gain[None],
        w_gate[0],
        w_up[0],
        w_down[0],
        new_state,
        far_outs=1,
    )
    parts = exchanged(parts.reshape(cores * tp_size, count, width), PLANE)
    (back,) = local_call(
        functools.partial(total_kernel, planes),
        [((planes, cores * capacity, width), BF16)],
        [],
        1 << 28,
        parts.reshape(cores, tp_size, count, width),
    )
    returned = exchanged(back, "z").reshape(expert_total * capacity, width)
    (layer_out,) = local_call(
        combine_kernel, [(wide, BF16)], [], 1 << 26, returned, slots, expert_weights.T, residual
    )
    return (layer_out, state_out[:, None])


def solution(mesh):
    axes = Mesh(mesh.devices.reshape(16, 2, 4, 4), ("z", "c", "y", "x"))
    ep = ("z", "c")
    in_specs = (
        P(ep, TP),
        P(ep, TP, None, None),
        P(),
        P(),
        P(None, TP),
        P(None, TP),
        P(None, TP),
        P(None, TP),
        P(),
        P(),
        P(TP),
        P(TP),
        P(),
        P(None, TP),
        P(ep, None),
        P(ep, None),
        P(ep, None, TP),
        P(ep, None, TP),
        P(ep, TP, None),
    )
    out_specs = (P(ep, TP), P(ep, TP, None, None))
    return jax.shard_map(shards, mesh=axes, in_specs=in_specs, out_specs=out_specs, check_vma=False)
```

```python
import functools

import jax
import jax.numpy as jnp
from jax import lax
from jax.experimental import pallas as pl
from jax.experimental.pallas import tpu as pltpu
from jax.sharding import Mesh, PartitionSpec as P

EPS = 1e-06
TP = ("y", "x")
PLANE = ("c", "y", "x")
BF16 = jnp.bfloat16
F32 = jnp.float32
VMEM_LIMIT = 12 << 20


def exchanged(blocks, axes):
    return lax.all_to_all(blocks, axes, 0, 0, tiled=True)


def silu(values):
    return values * (1.0 / (1.0 + jnp.exp(-values)))


def rounded(values):
    return values.astype(BF16).astype(F32)


def local_call(kernel, out_shapes, scratch, flops, *operands, far_outs=0):
    vmem = pl.BlockSpec(memory_space=pltpu.VMEM)
    outs = [jax.ShapeDtypeStruct(shape, dtype) for shape, dtype in out_shapes]
    return pl.pallas_call(
        kernel,
        out_shape=outs,
        in_specs=[vmem] * len(operands),
        out_specs=[vmem] * (len(outs) - far_outs) + [pl.BlockSpec(memory_space=pl.ANY)] * far_outs,
        scratch_shapes=scratch,
        compiler_params=pltpu.CompilerParams(vmem_limit_bytes=VMEM_LIMIT),
        cost_estimate=pl.CostEstimate(flops=flops, bytes_accessed=1 << 20, transcendentals=0),
    )(*operands)


def broadcast_kernel(shard, rate, shift, spread, rates):
    for tile in range(spread.shape[0]):
        spread[tile] = shard[...]
    row = lax.broadcasted_iota(jnp.int32, rates.shape, 0)
    rates[...] = jnp.where(row == 0, rate[...], shift[...])


def head_row(weight, head):
    values = weight[...].astype(F32)
    own = lax.broadcasted_iota(jnp.int32, values.shape, 0) == head
    return jnp.sum(jnp.where(own, values, 0.0), axis=0, keepdims=True)


def diagonal_masks(size):
    source = lax.broadcasted_iota(jnp.int32, (size, size), 0)
    target = lax.broadcasted_iota(jnp.int32, (size, size), 1)
    return source, target


def as_column(row):
    source, target = diagonal_masks(row.shape[1])
    return jnp.sum(jnp.where(source == target, row, 0.0), axis=1, keepdims=True)


def slot_rows(ids, expert_total, capacity):
    choices, seqs = ids.shape
    experts = lax.broadcasted_iota(jnp.int32, (expert_total, seqs), 0)
    chosen = [(ids[choice : choice + 1, :] == experts).astype(F32) for choice in range(choices)]
    source, target = diagonal_masks(seqs)
    before = (source < target).astype(F32).astype(BF16)
    earlier = jnp.dot((chosen[0] + chosen[1]).astype(BF16), before, preferred_element_type=F32)
    slots = []
    for choice in range(choices):
        rank = jnp.sum(earlier * chosen[choice], axis=0, keepdims=True).astype(jnp.int32)
        slots.append(ids[choice : choice + 1, :] * capacity + rank)
    return slots


def slot_hits(slots, slot_count):
    places = lax.broadcasted_iota(jnp.int32, (slot_count, slots[0].shape[1]), 0)
    return [(slot == places).astype(F32).astype(BF16) for slot in slots]


def lane_pair(left, right):
    shape = (left.shape[0], 128)
    lane = lax.broadcasted_iota(jnp.int32, shape, 1)
    return jnp.where(lane < 64, jnp.broadcast_to(left, shape), jnp.broadcast_to(right, shape))


def attend_kernel(tok, gain, wq, wk, wv, wg, w_decay, w_beta, head_gain, rates_in, state,
                  spread, new_state, normed, blocks, keys, from_key, from_query):
    tiles, seqs, width = tok.shape
    head_dim = wq.shape[0]
    half = seqs // 2
    for t in range(half):
        blocks[t] = jnp.concatenate([state[t], state[half + t]], axis=1)
    squares = jnp.zeros((seqs, width), F32)
    for tile in range(tiles):
        x = tok[tile].astype(F32)
        squares += x * x
    mean = jnp.sum(squares, axis=1, keepdims=True) / (tiles * width)
    scale = lax.rsqrt(mean + EPS)
    for tile in range(tiles):
        cols = slice(tile * width, (tile + 1) * width)
        normed[:, cols] = (tok[tile].astype(F32) * scale * gain[:, cols]).astype(BF16)
    rows = normed[...]
    dims = (((1,), (1,)), ((), ()))

    def unit(values):
        return values * lax.rsqrt(jnp.sum(values * values, axis=0, keepdims=True) + EPS)

    across = lax.dot_general(
        jnp.concatenate([wq[...], wk[...]], axis=0), rows, dims, preferred_element_type=F32
    )
    across = silu(rounded(across))
    query = unit(across[:head_dim]) * head_dim ** (-0.5)
    key = unit(across[head_dim:])
    both = jnp.concatenate([query, key], axis=0)
    high = rounded(both)
    terms = jnp.concatenate([high, both - high], axis=1).astype(BF16)
    token = lax.broadcasted_iota(jnp.int32, (seqs, 4 * head_dim), 0)
    lane = lax.broadcasted_iota(jnp.int32, (seqs, 4 * head_dim), 1)
    owner = jnp.where(lane % (2 * head_dim) < head_dim, token, token - half) - lane // (2 * head_dim)
    for t in range(0, half, 2):
        chosen = (owner == t).astype(F32).astype(BF16)
        repeated = jnp.dot(terms, jnp.concatenate([chosen, chosen], axis=0), preferred_element_type=F32)
        for step in range(2):
            row = t + step
            block = blocks[row]
            cols = slice(step * 2 * head_dim, (step + 1) * 2 * head_dim)
            key_pair = repeated[head_dim:, cols]
            keys[row] = key_pair
            from_key[row : row + 1, :] = jnp.sum(key_pair * block, axis=0, keepdims=True)
            from_query[row : row + 1, :] = jnp.sum(repeated[:head_dim, cols] * block, axis=0, keepdims=True)
    overlap = as_column(jnp.sum(query * key, axis=0, keepdims=True))
    overlap = lane_pair(overlap[:half], overlap[half:])
    own = lax.dot_general(rows, jnp.concatenate([wv[...], wg[...]], axis=0), dims, preferred_element_type=F32)
    own = silu(rounded(own))
    upper, lower = own[:half], own[half:]
    left = lax.broadcasted_iota(jnp.int32, upper.shape, 1) < head_dim
    value = jnp.where(left, upper, pltpu.roll(lower, head_dim, 1))
    gate = jnp.where(left, pltpu.roll(upper, head_dim, 1), lower)
    head = lax.axis_index("y") * lax.axis_size("x") + lax.axis_index("x")
    place = lax.broadcasted_iota(jnp.int32, (8, tiles * width), 0)
    w_rates = jnp.where(place == 0, head_row(w_decay, head), jnp.where(place == 1, head_row(w_beta, head), 0.0))
    rates = lax.dot_general(rows, w_rates.astype(BF16), dims, preferred_element_type=F32)
    decay_in = lane_pair(rates[:half, 0:1], rates[half:, 0:1]) + rates_in[1:2, :]
    soft = jnp.maximum(decay_in, 0.0) + jnp.log1p(jnp.exp(-jnp.abs(decay_in)))
    keep = jnp.exp(-rates_in[0:1, :] * soft)
    beta = 1.0 / (1.0 + jnp.exp(-lane_pair(rates[:half, 1:2], rates[half:, 1:2])))
    corr = beta * (value - keep * from_key[...])
    reading = keep * from_query[...] + overlap * corr
    squared = reading * reading
    means = [
        jnp.sum(jnp.where(side, squared, 0.0), axis=1, keepdims=True) / head_dim
        for side in (left, jnp.logical_not(left))
    ]
    reading_scale = lane_pair(lax.rsqrt(means[0] + EPS), lax.rsqrt(means[1] + EPS))
    gain_pair = jnp.concatenate([head_gain[...], head_gain[...]], axis=1)
    head_out = (reading * reading_scale * gain_pair * gate).astype(BF16)
    for tile in range(tiles):
        spread[tile] = head_out
    for t in range(half):
        updated = keep[t : t + 1, :] * blocks[t] + keys[t] * corr[t : t + 1, :]
        new_state[t] = updated[:, :head_dim]
        new_state[half + t] = updated[:, head_dim:]


def mix_kernel(expert_total, heads, w_mix, tokens, ids, residual, outgoing, slots_out):
    tiles, half, width = heads.shape
    top, bottom = [], []
    for pair in range(tiles // 2):
        even, odd = heads[2 * pair].astype(F32), heads[2 * pair + 1].astype(F32)
        left = lax.broadcasted_iota(jnp.int32, even.shape, 1) < width // 2
        top.append(jnp.where(left, even, pltpu.roll(odd, width // 2, 1)))
        bottom.append(jnp.where(left, pltpu.roll(even, width // 2, 1), odd))
    rows = [jnp.concatenate(part, axis=1).astype(BF16) for part in (top, bottom)]
    mixed = jnp.dot(jnp.concatenate(rows, axis=0), w_mix[...], preferred_element_type=F32)
    own = (tokens[...].astype(F32) + mixed).astype(BF16)
    residual[...] = own
    slots = slot_rows(ids, expert_total, outgoing.shape[0] // expert_total)
    for choice, slot in enumerate(slots):
        slots_out[choice : choice + 1, :] = slot
    first, second = slot_hits(slots, outgoing.shape[0])
    outgoing[...] = jnp.dot(first + second, own, preferred_element_type=F32).astype(BF16)


def spread_kernel(along_z, spread):
    planes = along_z.shape[0]
    cores, tiles, count, width = spread.shape
    capacity = count // planes
    rows = [along_z[plane].astype(F32) for plane in range(planes)]
    for core in range(cores):
        own = [row[core * capacity : (core + 1) * capacity] for row in rows]
        block = jnp.concatenate(own, axis=0).astype(BF16)
        for tile in range(tiles):
            spread[core, tile] = block


def expert_kernel(arrived, gain, w_gate, w_up, w_down, state, parts, state_out, normed, sem):
    state_copy = pltpu.make_async_copy(state, state_out, sem)
    state_copy.start()
    cores, tiles, count, width = arrived.shape
    for core in range(cores):
        squares = jnp.zeros((count, width), F32)
        for tile in range(tiles):
            x = arrived[core, tile].astype(F32)
            squares += x * x
        mean = jnp.sum(squares, axis=1, keepdims=True) / (tiles * width)
        scale = lax.rsqrt(mean + EPS)
        for tile in range(tiles):
            cols = slice(tile * width, (tile + 1) * width)
            x = arrived[core, tile].astype(F32) * scale * gain[:, cols]
            normed[core * count : (core + 1) * count, cols] = x.astype(BF16)
    rows = normed[...]
    gate = jnp.dot(rows, w_gate[...], preferred_element_type=F32)
    up = jnp.dot(rows, w_up[...], preferred_element_type=F32)
    hidden = (silu(gate) * up).astype(BF16)
    for pair in range(tiles // 2):
        cols = slice(2 * pair * width, 2 * (pair + 1) * width)
        part = jnp.dot(hidden, w_down[:, cols], preferred_element_type=F32).astype(BF16)
        for core in range(cores):
            own = part[core * count : (core + 1) * count]
            parts[core, 2 * pair] = own[:, :width]
            parts[core, 2 * pair + 1] = own[:, width:]
    state_copy.wait()


def total_kernel(planes, parts, back):
    cores, tiles, count, width = parts.shape
    capacity = count // planes
    sums = []
    for core in range(cores):
        total = parts[core, 0].astype(F32)
        for tile in range(1, tiles):
            total += parts[core, tile].astype(F32)
        sums.append(total)
    for plane in range(planes):
        own = [total[plane * capacity : (plane + 1) * capacity] for total in sums]
        back[plane] = jnp.concatenate(own, axis=0).astype(BF16)


def combine_kernel(returned, slots, weights, residual, layer_out):
    rows = returned[...]
    dims = (((0,), (0,)), ((), ()))
    weighted = residual[...].astype(F32)
    owners = [slots[choice : choice + 1, :] for choice in range(slots.shape[0])]
    for choice, hit in enumerate(slot_hits(owners, rows.shape[0])):
        pair = lax.dot_general(hit, rows, dims, preferred_element_type=F32)
        weighted += pair * as_column(weights[choice : choice + 1, :])
    layer_out[...] = weighted.astype(BF16)


def shards(
    tokens,
    state,
    attn_gain,
    ffn_gain,
    w_query,
    w_key,
    w_value,
    w_output_gate,
    w_decay,
    w_beta,
    decay_rate,
    decay_shift,
    head_gain,
    w_mix_out,
    expert_ids,
    expert_weights,
    w_gate,
    w_up,
    w_down,
):
    planes = lax.axis_size("z")
    cores = lax.axis_size("c")
    tp_size = lax.axis_size(TP)
    seqs, width = tokens.shape
    head_dim = head_gain.shape[0]
    model_width = attn_gain.shape[0]
    top_count = expert_ids.shape[1]
    expert_total = planes * cores
    capacity = 2 * seqs * top_count // expert_total
    half = seqs // 2
    count = planes * capacity

    slot_count = expert_total * capacity
    wide = (seqs, width)
    token_spread, head_rates = local_call(
        broadcast_kernel,
        [((tp_size, *wide), BF16), ((2, 2 * head_dim), F32)],
        [],
        1 << 35,
        tokens,
        decay_rate[None],
        decay_shift[None],
    )
    gathered = exchanged(token_spread, TP)
    square = (half, 2 * head_dim)
    blocks = (half, head_dim, 2 * head_dim)
    spread, new_state = local_call(
        attend_kernel,
        [((tp_size, *square), BF16), ((seqs, head_dim, head_dim), F32)],
        [
            pltpu.VMEM((seqs, model_width), BF16),
            pltpu.VMEM(blocks, F32),
            pltpu.VMEM(blocks, F32),
            pltpu.VMEM(square, F32),
            pltpu.VMEM(square, F32),
        ],
        1 << 30,
        gathered,
        attn_gain[None],
        w_query.T,
        w_key.T,
        w_value.T,
        w_output_gate.T,
        w_decay.T,
        w_beta.T,
        head_gain[None],
        head_rates,
        state[:, 0],
    )
    heads = exchanged(spread, TP)
    residual, outgoing, slots = local_call(
        functools.partial(mix_kernel, expert_total),
        [(wide, BF16), ((slot_count, width), BF16), ((top_count, seqs), jnp.int32)],
        [],
        1 << 28,
        heads,
        w_mix_out,
        tokens,
        expert_ids.T,
    )
    along_z = exchanged(outgoing.reshape(planes, cores * capacity, width), "z")
    (spread_rows,) = local_call(
        spread_kernel, [((cores, tp_size, count, width), BF16)], [], 1 << 28, along_z
    )
    arrived = exchanged(spread_rows.reshape(cores * tp_size, count, width), PLANE)
    parts, state_out = local_call(
        expert_kernel,
        [((cores, tp_size, count, width), BF16), (new_state.shape, F32)],
        [pltpu.VMEM((cores * count, model_width), BF16), pltpu.SemaphoreType.DMA],
        1 << 30,
        arrived.reshape(cores, tp_size, count, width),
        ffn_gain[None],
        w_gate[0],
        w_up[0],
        w_down[0],
        new_state,
        far_outs=1,
    )
    parts = exchanged(parts.reshape(cores * tp_size, count, width), PLANE)
    (back,) = local_call(
        functools.partial(total_kernel, planes),
        [((planes, cores * capacity, width), BF16)],
        [],
        1 << 28,
        parts.reshape(cores, tp_size, count, width),
    )
    returned = exchanged(back, "z").reshape(expert_total * capacity, width)
    (layer_out,) = local_call(
        combine_kernel, [(wide, BF16)], [], 1 << 26, returned, slots, expert_weights.T, residual
    )
    return (layer_out, state_out[:, None])


def solution(mesh):
    axes = Mesh(mesh.devices.reshape(16, 2, 4, 4), ("z", "c", "y", "x"))
    ep = ("z", "c")
    in_specs = (
        P(ep, TP),
        P(ep, TP, None, None),
        P(),
        P(),
        P(None, TP),
        P(None, TP),
        P(None, TP),
        P(None, TP),
        P(),
        P(),
        P(TP),
        P(TP),
        P(),
        P(None, TP),
        P(ep, None),
        P(ep, None),
        P(ep, None, TP),
        P(ep, None, TP),
        P(ep, TP, None),
    )
    out_specs = (P(ep, TP), P(ep, TP, None, None))
    return jax.shard_map(shards, mesh=axes, in_specs=in_specs, out_specs=out_specs, check_vma=False)
```

```python
import functools

import jax
import jax.numpy as jnp
from jax import lax
from jax.experimental import pallas as pl
from jax.experimental.pallas import tpu as pltpu
from jax.sharding import Mesh, PartitionSpec as P

EPS = 1e-06
TP = ("y", "x")
PLANE = ("c", "y", "x")
BF16 = jnp.bfloat16
F32 = jnp.float32
VMEM_LIMIT = 12 << 20


def exchanged(blocks, axes):
    return lax.all_to_all(blocks, axes, 0, 0, tiled=True)


def silu(values):
    return values * (1.0 / (1.0 + jnp.exp(-values)))


def rounded(values):
    return values.astype(BF16).astype(F32)


def local_call(kernel, out_shapes, scratch, flops, *operands, far_outs=0):
    vmem = pl.BlockSpec(memory_space=pltpu.VMEM)
    outs = [jax.ShapeDtypeStruct(shape, dtype) for shape, dtype in out_shapes]
    return pl.pallas_call(
        kernel,
        out_shape=outs,
        in_specs=[vmem] * len(operands),
        out_specs=[vmem] * (len(outs) - far_outs) + [pl.BlockSpec(memory_space=pl.ANY)] * far_outs,
        scratch_shapes=scratch,
        compiler_params=pltpu.CompilerParams(vmem_limit_bytes=VMEM_LIMIT),
        cost_estimate=pl.CostEstimate(flops=flops, bytes_accessed=1 << 20, transcendentals=0),
    )(*operands)


def owner_kernel(owner):
    seqs, columns = owner.shape
    token = lax.broadcasted_iota(jnp.int32, owner.shape, 0)
    lane = lax.broadcasted_iota(jnp.int32, owner.shape, 1)
    row = columns // 2
    owner[...] = jnp.where(lane % row < row // 2, token, token - seqs // 2) - lane // row


def broadcast_kernel(shard, rate, shift, owner, spread, rates, owner_out):
    owner_out[...] = owner[...]
    for tile in range(spread.shape[0]):
        spread[tile] = shard[...]
    row = lax.broadcasted_iota(jnp.int32, rates.shape, 0)
    rates[...] = jnp.where(row == 0, rate[...], shift[...])


def head_row(weight, head):
    values = weight[...].astype(F32)
    own = lax.broadcasted_iota(jnp.int32, values.shape, 0) == head
    return jnp.sum(jnp.where(own, values, 0.0), axis=0, keepdims=True)


def diagonal_masks(size):
    source = lax.broadcasted_iota(jnp.int32, (size, size), 0)
    target = lax.broadcasted_iota(jnp.int32, (size, size), 1)
    return source, target


def as_column(row):
    source, target = diagonal_masks(row.shape[1])
    return jnp.sum(jnp.where(source == target, row, 0.0), axis=1, keepdims=True)


def slot_rows(ids, expert_total, capacity):
    choices, seqs = ids.shape
    experts = lax.broadcasted_iota(jnp.int32, (expert_total, seqs), 0)
    chosen = [(ids[choice : choice + 1, :] == experts).astype(F32) for choice in range(choices)]
    source, target = diagonal_masks(seqs)
    before = (source < target).astype(F32).astype(BF16)
    earlier = jnp.dot((chosen[0] + chosen[1]).astype(BF16), before, preferred_element_type=F32)
    slots = []
    for choice in range(choices):
        rank = jnp.sum(earlier * chosen[choice], axis=0, keepdims=True).astype(jnp.int32)
        slots.append(ids[choice : choice + 1, :] * capacity + rank)
    return slots


def slot_hits(slots, slot_count):
    places = lax.broadcasted_iota(jnp.int32, (slot_count, slots[0].shape[1]), 0)
    return [(slot == places).astype(F32).astype(BF16) for slot in slots]


def lane_pair(left, right):
    shape = (left.shape[0], 128)
    lane = lax.broadcasted_iota(jnp.int32, shape, 1)
    return jnp.where(lane < 64, jnp.broadcast_to(left, shape), jnp.broadcast_to(right, shape))


def attend_kernel(tok, gain, wq, wk, wv, wg, w_decay, w_beta, head_gain, rates_in, owner, state,
                  spread, new_state, normed, blocks, keys, from_key, from_query):
    tiles, seqs, width = tok.shape
    head_dim = wq.shape[0]
    half = seqs // 2
    for t in range(half):
        blocks[t] = jnp.concatenate([state[t], state[half + t]], axis=1)
    squares = jnp.zeros((seqs, width), F32)
    for tile in range(tiles):
        x = tok[tile].astype(F32)
        squares += x * x
    mean = jnp.sum(squares, axis=1, keepdims=True) / (tiles * width)
    scale = lax.rsqrt(mean + EPS)
    for tile in range(tiles):
        cols = slice(tile * width, (tile + 1) * width)
        normed[:, cols] = (tok[tile].astype(F32) * scale * gain[:, cols]).astype(BF16)
    rows = normed[...]
    dims = (((1,), (1,)), ((), ()))

    def unit(values):
        return values * lax.rsqrt(jnp.sum(values * values, axis=0, keepdims=True) + EPS)

    across = lax.dot_general(
        jnp.concatenate([wq[...], wk[...]], axis=0), rows, dims, preferred_element_type=F32
    )
    across = silu(rounded(across))
    query = unit(across[:head_dim]) * head_dim ** (-0.5)
    key = unit(across[head_dim:])
    both = jnp.concatenate([query, key], axis=0)
    high = rounded(both)
    terms = jnp.concatenate([high, both - high], axis=1).astype(BF16)
    for t in range(0, half, 2):
        chosen = (owner[...] == t).astype(F32).astype(BF16)
        repeated = jnp.dot(terms, jnp.concatenate([chosen, chosen], axis=0), preferred_element_type=F32)
        for step in range(2):
            row = t + step
            block = blocks[row]
            cols = slice(step * 2 * head_dim, (step + 1) * 2 * head_dim)
            key_pair = repeated[head_dim:, cols]
            keys[row] = key_pair
            from_key[row : row + 1, :] = jnp.sum(key_pair * block, axis=0, keepdims=True)
            from_query[row : row + 1, :] = jnp.sum(repeated[:head_dim, cols] * block, axis=0, keepdims=True)
    overlap = as_column(jnp.sum(query * key, axis=0, keepdims=True))
    overlap = lane_pair(overlap[:half], overlap[half:])
    own = lax.dot_general(rows, jnp.concatenate([wv[...], wg[...]], axis=0), dims, preferred_element_type=F32)
    own = silu(rounded(own))
    upper, lower = own[:half], own[half:]
    left = lax.broadcasted_iota(jnp.int32, upper.shape, 1) < head_dim
    value = jnp.where(left, upper, pltpu.roll(lower, head_dim, 1))
    gate = jnp.where(left, pltpu.roll(upper, head_dim, 1), lower)
    head = lax.axis_index("y") * lax.axis_size("x") + lax.axis_index("x")
    place = lax.broadcasted_iota(jnp.int32, (8, tiles * width), 0)
    w_rates = jnp.where(place == 0, head_row(w_decay, head), jnp.where(place == 1, head_row(w_beta, head), 0.0))
    rates = lax.dot_general(rows, w_rates.astype(BF16), dims, preferred_element_type=F32)
    decay_in = lane_pair(rates[:half, 0:1], rates[half:, 0:1]) + rates_in[1:2, :]
    soft = jnp.maximum(decay_in, 0.0) + jnp.log1p(jnp.exp(-jnp.abs(decay_in)))
    keep = jnp.exp(-rates_in[0:1, :] * soft)
    beta = 1.0 / (1.0 + jnp.exp(-lane_pair(rates[:half, 1:2], rates[half:, 1:2])))
    corr = beta * (value - keep * from_key[...])
    reading = keep * from_query[...] + overlap * corr
    squared = reading * reading
    means = [
        jnp.sum(jnp.where(side, squared, 0.0), axis=1, keepdims=True) / head_dim
        for side in (left, jnp.logical_not(left))
    ]
    reading_scale = lane_pair(lax.rsqrt(means[0] + EPS), lax.rsqrt(means[1] + EPS))
    gain_pair = jnp.concatenate([head_gain[...], head_gain[...]], axis=1)
    head_out = (reading * reading_scale * gain_pair * gate).astype(BF16)
    for tile in range(tiles):
        spread[tile] = head_out
    for t in range(half):
        updated = keep[t : t + 1, :] * blocks[t] + keys[t] * corr[t : t + 1, :]
        new_state[t] = updated[:, :head_dim]
        new_state[half + t] = updated[:, head_dim:]


def mix_kernel(expert_total, heads, w_mix, tokens, ids, residual, outgoing, slots_out):
    tiles, half, width = heads.shape
    top, bottom = [], []
    for pair in range(tiles // 2):
        even, odd = heads[2 * pair].astype(F32), heads[2 * pair + 1].astype(F32)
        left = lax.broadcasted_iota(jnp.int32, even.shape, 1) < width // 2
        top.append(jnp.where(left, even, pltpu.roll(odd, width // 2, 1)))
        bottom.append(jnp.where(left, pltpu.roll(even, width // 2, 1), odd))
    rows = [jnp.concatenate(part, axis=1).astype(BF16) for part in (top, bottom)]
    mixed = jnp.dot(jnp.concatenate(rows, axis=0), w_mix[...], preferred_element_type=F32)
    own = (tokens[...].astype(F32) + mixed).astype(BF16)
    residual[...] = own
    slots = slot_rows(ids, expert_total, outgoing.shape[0] // expert_total)
    for choice, slot in enumerate(slots):
        slots_out[choice : choice + 1, :] = slot
    first, second = slot_hits(slots, outgoing.shape[0])
    outgoing[...] = jnp.dot(first + second, own, preferred_element_type=F32).astype(BF16)


def spread_kernel(along_z, spread):
    planes = along_z.shape[0]
    cores, tiles, count, width = spread.shape
    capacity = count // planes
    rows = [along_z[plane].astype(F32) for plane in range(planes)]
    for core in range(cores):
        own = [row[core * capacity : (core + 1) * capacity] for row in rows]
        block = jnp.concatenate(own, axis=0).astype(BF16)
        for tile in range(tiles):
            spread[core, tile] = block


def expert_kernel(arrived, gain, w_gate, w_up, w_down, state, parts, state_out, normed, sem):
    state_copy = pltpu.make_async_copy(state, state_out, sem)
    state_copy.start()
    cores, tiles, count, width = arrived.shape
    for core in range(cores):
        squares = jnp.zeros((count, width), F32)
        for tile in range(tiles):
            x = arrived[core, tile].astype(F32)
            squares += x * x
        mean = jnp.sum(squares, axis=1, keepdims=True) / (tiles * width)
        scale = lax.rsqrt(mean + EPS)
        for tile in range(tiles):
            cols = slice(tile * width, (tile + 1) * width)
            x = arrived[core, tile].astype(F32) * scale * gain[:, cols]
            normed[core * count : (core + 1) * count, cols] = x.astype(BF16)
    rows = normed[...]
    gate = jnp.dot(rows, w_gate[...], preferred_element_type=F32)
    up = jnp.dot(rows, w_up[...], preferred_element_type=F32)
    hidden = (silu(gate) * up).astype(BF16)
    for pair in range(tiles // 2):
        cols = slice(2 * pair * width, 2 * (pair + 1) * width)
        part = jnp.dot(hidden, w_down[:, cols], preferred_element_type=F32).astype(BF16)
        for core in range(cores):
            own = part[core * count : (core + 1) * count]
            parts[core, 2 * pair] = own[:, :width]
            parts[core, 2 * pair + 1] = own[:, width:]
    state_copy.wait()


def total_kernel(planes, parts, back):
    cores, tiles, count, width = parts.shape
    capacity = count // planes
    sums = []
    for core in range(cores):
        total = parts[core, 0].astype(F32)
        for tile in range(1, tiles):
            total += parts[core, tile].astype(F32)
        sums.append(total)
    for plane in range(planes):
        own = [total[plane * capacity : (plane + 1) * capacity] for total in sums]
        back[plane] = jnp.concatenate(own, axis=0).astype(BF16)


def combine_kernel(returned, slots, weights, residual, layer_out):
    rows = returned[...]
    dims = (((0,), (0,)), ((), ()))
    weighted = residual[...].astype(F32)
    owners = [slots[choice : choice + 1, :] for choice in range(slots.shape[0])]
    for choice, hit in enumerate(slot_hits(owners, rows.shape[0])):
        pair = lax.dot_general(hit, rows, dims, preferred_element_type=F32)
        weighted += pair * as_column(weights[choice : choice + 1, :])
    layer_out[...] = weighted.astype(BF16)


def shards(
    tokens,
    state,
    attn_gain,
    ffn_gain,
    w_query,
    w_key,
    w_value,
    w_output_gate,
    w_decay,
    w_beta,
    decay_rate,
    decay_shift,
    head_gain,
    w_mix_out,
    expert_ids,
    expert_weights,
    w_gate,
    w_up,
    w_down,
):
    planes = lax.axis_size("z")
    cores = lax.axis_size("c")
    tp_size = lax.axis_size(TP)
    seqs, width = tokens.shape
    head_dim = head_gain.shape[0]
    model_width = attn_gain.shape[0]
    top_count = expert_ids.shape[1]
    expert_total = planes * cores
    capacity = 2 * seqs * top_count // expert_total
    half = seqs // 2
    count = planes * capacity

    slot_count = expert_total * capacity
    wide = (seqs, width)
    (owner,) = local_call(owner_kernel, [((seqs, 4 * head_dim), jnp.int32)], [], 1 << 35)
    token_spread, head_rates, owner = local_call(
        broadcast_kernel,
        [((tp_size, *wide), BF16), ((2, 2 * head_dim), F32), (owner.shape, jnp.int32)],
        [],
        1 << 35,
        tokens,
        decay_rate[None],
        decay_shift[None],
        owner,
    )
    gathered = exchanged(token_spread, TP)
    square = (half, 2 * head_dim)
    blocks = (half, head_dim, 2 * head_dim)
    spread, new_state = local_call(
        attend_kernel,
        [((tp_size, *square), BF16), ((seqs, head_dim, head_dim), F32)],
        [
            pltpu.VMEM((seqs, model_width), BF16),
            pltpu.VMEM(blocks, F32),
            pltpu.VMEM(blocks, F32),
            pltpu.VMEM(square, F32),
            pltpu.VMEM(square, F32),
        ],
        1 << 30,
        gathered,
        attn_gain[None],
        w_query.T,
        w_key.T,
        w_value.T,
        w_output_gate.T,
        w_decay.T,
        w_beta.T,
        head_gain[None],
        head_rates,
        owner,
        state[:, 0],
    )
    heads = exchanged(spread, TP)
    residual, outgoing, slots = local_call(
        functools.partial(mix_kernel, expert_total),
        [(wide, BF16), ((slot_count, width), BF16), ((top_count, seqs), jnp.int32)],
        [],
        1 << 28,
        heads,
        w_mix_out,
        tokens,
        expert_ids.T,
    )
    along_z = exchanged(outgoing.reshape(planes, cores * capacity, width), "z")
    (spread_rows,) = local_call(
        spread_kernel, [((cores, tp_size, count, width), BF16)], [], 1 << 28, along_z
    )
    arrived = exchanged(spread_rows.reshape(cores * tp_size, count, width), PLANE)
    parts, state_out = local_call(
        expert_kernel,
        [((cores, tp_size, count, width), BF16), (new_state.shape, F32)],
        [pltpu.VMEM((cores * count, model_width), BF16), pltpu.SemaphoreType.DMA],
        1 << 30,
        arrived.reshape(cores, tp_size, count, width),
        ffn_gain[None],
        w_gate[0],
        w_up[0],
        w_down[0],
        new_state,
        far_outs=1,
    )
    parts = exchanged(parts.reshape(cores * tp_size, count, width), PLANE)
    (back,) = local_call(
        functools.partial(total_kernel, planes),
        [((planes, cores * capacity, width), BF16)],
        [],
        1 << 28,
        parts.reshape(cores, tp_size, count, width),
    )
    returned = exchanged(back, "z").reshape(expert_total * capacity, width)
    (layer_out,) = local_call(
        combine_kernel, [(wide, BF16)], [], 1 << 26, returned, slots, expert_weights.T, residual
    )
    return (layer_out, state_out[:, None])


def solution(mesh):
    axes = Mesh(mesh.devices.reshape(16, 2, 4, 4), ("z", "c", "y", "x"))
    ep = ("z", "c")
    in_specs = (
        P(ep, TP),
        P(ep, TP, None, None),
        P(),
        P(),
        P(None, TP),
        P(None, TP),
        P(None, TP),
        P(None, TP),
        P(),
        P(),
        P(TP),
        P(TP),
        P(),
        P(None, TP),
        P(ep, None),
        P(ep, None),
        P(ep, None, TP),
        P(ep, None, TP),
        P(ep, TP, None),
    )
    out_specs = (P(ep, TP), P(ep, TP, None, None))
    return jax.shard_map(shards, mesh=axes, in_specs=in_specs, out_specs=out_specs, check_vma=False)
```

```python
import functools

import jax
import jax.numpy as jnp
from jax import lax
from jax.experimental import pallas as pl
from jax.experimental.pallas import tpu as pltpu
from jax.sharding import Mesh, PartitionSpec as P

EPS = 1e-06
TP = ("y", "x")
PLANE = ("c", "y", "x")
BF16 = jnp.bfloat16
F32 = jnp.float32
VMEM_LIMIT = 12 << 20


def exchanged(blocks, axes):
    return lax.all_to_all(blocks, axes, 0, 0, tiled=True)


def silu(values):
    return values * (1.0 / (1.0 + jnp.exp(-values)))


def rounded(values):
    return values.astype(BF16).astype(F32)


def local_call(kernel, out_shapes, scratch, flops, *operands, far_outs=0):
    vmem = pl.BlockSpec(memory_space=pltpu.VMEM)
    outs = [jax.ShapeDtypeStruct(shape, dtype) for shape, dtype in out_shapes]
    return pl.pallas_call(
        kernel,
        out_shape=outs,
        in_specs=[vmem] * len(operands),
        out_specs=[vmem] * (len(outs) - far_outs) + [pl.BlockSpec(memory_space=pl.ANY)] * far_outs,
        scratch_shapes=scratch,
        compiler_params=pltpu.CompilerParams(vmem_limit_bytes=VMEM_LIMIT),
        cost_estimate=pl.CostEstimate(flops=flops, bytes_accessed=1 << 20, transcendentals=0),
    )(*operands)


def owner_kernel(owner):
    seqs, columns = owner.shape
    token = lax.broadcasted_iota(jnp.int32, owner.shape, 0)
    lane = lax.broadcasted_iota(jnp.int32, owner.shape, 1)
    row = columns // 2
    owner[...] = jnp.where(lane % row < row // 2, token, token - seqs // 2) - lane // row


def broadcast_kernel(shard, rate, shift, owner, spread, rates, owner_out):
    owner_out[...] = owner[...]
    for tile in range(spread.shape[0]):
        spread[tile] = shard[...]
    row = lax.broadcasted_iota(jnp.int32, rates.shape, 0)
    rates[...] = jnp.where(row == 0, rate[...], shift[...])


def head_row(weight, head):
    values = weight[...].astype(F32)
    own = lax.broadcasted_iota(jnp.int32, values.shape, 0) == head
    return jnp.sum(jnp.where(own, values, 0.0), axis=0, keepdims=True)


def diagonal_masks(size):
    source = lax.broadcasted_iota(jnp.int32, (size, size), 0)
    target = lax.broadcasted_iota(jnp.int32, (size, size), 1)
    return source, target


def as_column(row):
    source, target = diagonal_masks(row.shape[1])
    return jnp.sum(jnp.where(source == target, row, 0.0), axis=1, keepdims=True)


def slot_rows(ids, expert_total, capacity):
    choices, seqs = ids.shape
    experts = lax.broadcasted_iota(jnp.int32, (expert_total, seqs), 0)
    chosen = [(ids[choice : choice + 1, :] == experts).astype(F32) for choice in range(choices)]
    source, target = diagonal_masks(seqs)
    before = (source < target).astype(F32).astype(BF16)
    earlier = jnp.dot((chosen[0] + chosen[1]).astype(BF16), before, preferred_element_type=F32)
    slots = []
    for choice in range(choices):
        rank = jnp.sum(earlier * chosen[choice], axis=0, keepdims=True).astype(jnp.int32)
        slots.append(ids[choice : choice + 1, :] * capacity + rank)
    return slots


def slot_hits(slots, slot_count):
    places = lax.broadcasted_iota(jnp.int32, (slot_count, slots[0].shape[1]), 0)
    return [(slot == places).astype(F32).astype(BF16) for slot in slots]


def lane_pair(left, right):
    shape = (left.shape[0], 128)
    lane = lax.broadcasted_iota(jnp.int32, shape, 1)
    return jnp.where(lane < 64, jnp.broadcast_to(left, shape), jnp.broadcast_to(right, shape))


def attend_kernel(tok, gain, wq, wk, wv, wg, w_decay, w_beta, head_gain, rates_in, owner, state,
                  spread, new_state, normed, blocks, keys, from_key, from_query):
    tiles, seqs, width = tok.shape
    head_dim = wq.shape[0]
    half = seqs // 2
    for t in range(half):
        blocks[t] = jnp.concatenate([state[t], state[half + t]], axis=1)
    squares = jnp.zeros((seqs, width), F32)
    for tile in range(tiles):
        x = tok[tile].astype(F32)
        squares += x * x
    mean = jnp.sum(squares, axis=1, keepdims=True) / (tiles * width)
    scale = lax.rsqrt(mean + EPS)
    for tile in range(tiles):
        cols = slice(tile * width, (tile + 1) * width)
        normed[:, cols] = (tok[tile].astype(F32) * scale * gain[:, cols]).astype(BF16)
    rows = normed[...]
    dims = (((1,), (1,)), ((), ()))

    def unit(values):
        return values * lax.rsqrt(jnp.sum(values * values, axis=0, keepdims=True) + EPS)

    across = lax.dot_general(
        jnp.concatenate([wq[...], wk[...]], axis=0), rows, dims, preferred_element_type=F32
    )
    across = silu(rounded(across))
    query = unit(across[:head_dim]) * head_dim ** (-0.5)
    key = unit(across[head_dim:])
    overlap = as_column(jnp.sum(query * key, axis=0, keepdims=True))
    overlap = lane_pair(overlap[:half], overlap[half:])
    own = lax.dot_general(rows, jnp.concatenate([wv[...], wg[...]], axis=0), dims, preferred_element_type=F32)
    own = silu(rounded(own))
    upper, lower = own[:half], own[half:]
    left = lax.broadcasted_iota(jnp.int32, upper.shape, 1) < head_dim
    value = jnp.where(left, upper, pltpu.roll(lower, head_dim, 1))
    gate = jnp.where(left, pltpu.roll(upper, head_dim, 1), lower)
    head = lax.axis_index("y") * lax.axis_size("x") + lax.axis_index("x")
    place = lax.broadcasted_iota(jnp.int32, (8, tiles * width), 0)
    w_rates = jnp.where(place == 0, head_row(w_decay, head), jnp.where(place == 1, head_row(w_beta, head), 0.0))
    rates = lax.dot_general(rows, w_rates.astype(BF16), dims, preferred_element_type=F32)
    decay_in = lane_pair(rates[:half, 0:1], rates[half:, 0:1]) + rates_in[1:2, :]
    soft = jnp.maximum(decay_in, 0.0) + jnp.log1p(jnp.exp(-jnp.abs(decay_in)))
    keep = jnp.exp(-rates_in[0:1, :] * soft)
    beta = 1.0 / (1.0 + jnp.exp(-lane_pair(rates[:half, 1:2], rates[half:, 1:2])))
    both = jnp.concatenate([query, key], axis=0)
    high = rounded(both)
    terms = jnp.concatenate([high, both - high], axis=1).astype(BF16)
    for t in range(0, half, 2):
        chosen = (owner[...] == t).astype(F32).astype(BF16)
        repeated = jnp.dot(terms, jnp.concatenate([chosen, chosen], axis=0), preferred_element_type=F32)
        for step in range(2):
            row = t + step
            block = blocks[row]
            cols = slice(step * 2 * head_dim, (step + 1) * 2 * head_dim)
            key_pair = repeated[head_dim:, cols]
            keys[row] = key_pair
            from_key[row : row + 1, :] = jnp.sum(key_pair * block, axis=0, keepdims=True)
            from_query[row : row + 1, :] = jnp.sum(repeated[:head_dim, cols] * block, axis=0, keepdims=True)
    corr = beta * (value - keep * from_key[...])
    reading = keep * from_query[...] + overlap * corr
    squared = reading * reading
    means = [
        jnp.sum(jnp.where(side, squared, 0.0), axis=1, keepdims=True) / head_dim
        for side in (left, jnp.logical_not(left))
    ]
    reading_scale = lane_pair(lax.rsqrt(means[0] + EPS), lax.rsqrt(means[1] + EPS))
    gain_pair = jnp.concatenate([head_gain[...], head_gain[...]], axis=1)
    head_out = (reading * reading_scale * gain_pair * gate).astype(BF16)
    for tile in range(tiles):
        spread[tile] = head_out
    for t in range(half):
        updated = keep[t : t + 1, :] * blocks[t] + keys[t] * corr[t : t + 1, :]
        new_state[t] = updated[:, :head_dim]
        new_state[half + t] = updated[:, head_dim:]


def mix_kernel(expert_total, heads, w_mix, tokens, ids, residual, outgoing, slots_out):
    tiles, half, width = heads.shape
    top, bottom = [], []
    for pair in range(tiles // 2):
        even, odd = heads[2 * pair].astype(F32), heads[2 * pair + 1].astype(F32)
        left = lax.broadcasted_iota(jnp.int32, even.shape, 1) < width // 2
        top.append(jnp.where(left, even, pltpu.roll(odd, width // 2, 1)))
        bottom.append(jnp.where(left, pltpu.roll(even, width // 2, 1), odd))
    rows = [jnp.concatenate(part, axis=1).astype(BF16) for part in (top, bottom)]
    mixed = jnp.dot(jnp.concatenate(rows, axis=0), w_mix[...], preferred_element_type=F32)
    own = (tokens[...].astype(F32) + mixed).astype(BF16)
    residual[...] = own
    slots = slot_rows(ids, expert_total, outgoing.shape[0] // expert_total)
    for choice, slot in enumerate(slots):
        slots_out[choice : choice + 1, :] = slot
    first, second = slot_hits(slots, outgoing.shape[0])
    outgoing[...] = jnp.dot(first + second, own, preferred_element_type=F32).astype(BF16)


def spread_kernel(along_z, spread):
    planes = along_z.shape[0]
    cores, tiles, count, width = spread.shape
    capacity = count // planes
    rows = [along_z[plane].astype(F32) for plane in range(planes)]
    for core in range(cores):
        own = [row[core * capacity : (core + 1) * capacity] for row in rows]
        block = jnp.concatenate(own, axis=0).astype(BF16)
        for tile in range(tiles):
            spread[core, tile] = block


def expert_kernel(arrived, gain, w_gate, w_up, w_down, state, parts, state_out, normed, sem):
    state_copy = pltpu.make_async_copy(state, state_out, sem)
    state_copy.start()
    cores, tiles, count, width = arrived.shape
    for core in range(cores):
        squares = jnp.zeros((count, width), F32)
        for tile in range(tiles):
            x = arrived[core, tile].astype(F32)
            squares += x * x
        mean = jnp.sum(squares, axis=1, keepdims=True) / (tiles * width)
        scale = lax.rsqrt(mean + EPS)
        for tile in range(tiles):
            cols = slice(tile * width, (tile + 1) * width)
            x = arrived[core, tile].astype(F32) * scale * gain[:, cols]
            normed[core * count : (core + 1) * count, cols] = x.astype(BF16)
    rows = normed[...]
    gate = jnp.dot(rows, w_gate[...], preferred_element_type=F32)
    up = jnp.dot(rows, w_up[...], preferred_element_type=F32)
    hidden = (silu(gate) * up).astype(BF16)
    for pair in range(tiles // 2):
        cols = slice(2 * pair * width, 2 * (pair + 1) * width)
        part = jnp.dot(hidden, w_down[:, cols], preferred_element_type=F32).astype(BF16)
        for core in range(cores):
            own = part[core * count : (core + 1) * count]
            parts[core, 2 * pair] = own[:, :width]
            parts[core, 2 * pair + 1] = own[:, width:]
    state_copy.wait()


def total_kernel(planes, parts, back):
    cores, tiles, count, width = parts.shape
    capacity = count // planes
    sums = []
    for core in range(cores):
        total = parts[core, 0].astype(F32)
        for tile in range(1, tiles):
            total += parts[core, tile].astype(F32)
        sums.append(total)
    for plane in range(planes):
        own = [total[plane * capacity : (plane + 1) * capacity] for total in sums]
        back[plane] = jnp.concatenate(own, axis=0).astype(BF16)


def combine_kernel(returned, slots, weights, residual, layer_out):
    rows = returned[...]
    dims = (((0,), (0,)), ((), ()))
    weighted = residual[...].astype(F32)
    owners = [slots[choice : choice + 1, :] for choice in range(slots.shape[0])]
    for choice, hit in enumerate(slot_hits(owners, rows.shape[0])):
        pair = lax.dot_general(hit, rows, dims, preferred_element_type=F32)
        weighted += pair * as_column(weights[choice : choice + 1, :])
    layer_out[...] = weighted.astype(BF16)


def shards(
    tokens,
    state,
    attn_gain,
    ffn_gain,
    w_query,
    w_key,
    w_value,
    w_output_gate,
    w_decay,
    w_beta,
    decay_rate,
    decay_shift,
    head_gain,
    w_mix_out,
    expert_ids,
    expert_weights,
    w_gate,
    w_up,
    w_down,
):
    planes = lax.axis_size("z")
    cores = lax.axis_size("c")
    tp_size = lax.axis_size(TP)
    seqs, width = tokens.shape
    head_dim = head_gain.shape[0]
    model_width = attn_gain.shape[0]
    top_count = expert_ids.shape[1]
    expert_total = planes * cores
    capacity = 2 * seqs * top_count // expert_total
    half = seqs // 2
    count = planes * capacity

    slot_count = expert_total * capacity
    wide = (seqs, width)
    (owner,) = local_call(owner_kernel, [((seqs, 4 * head_dim), jnp.int32)], [], 1 << 35)
    token_spread, head_rates, owner = local_call(
        broadcast_kernel,
        [((tp_size, *wide), BF16), ((2, 2 * head_dim), F32), (owner.shape, jnp.int32)],
        [],
        1 << 35,
        tokens,
        decay_rate[None],
        decay_shift[None],
        owner,
    )
    gathered = exchanged(token_spread, TP)
    square = (half, 2 * head_dim)
    blocks = (half, head_dim, 2 * head_dim)
    spread, new_state = local_call(
        attend_kernel,
        [((tp_size, *square), BF16), ((seqs, head_dim, head_dim), F32)],
        [
            pltpu.VMEM((seqs, model_width), BF16),
            pltpu.VMEM(blocks, F32),
            pltpu.VMEM(blocks, F32),
            pltpu.VMEM(square, F32),
            pltpu.VMEM(square, F32),
        ],
        1 << 30,
        gathered,
        attn_gain[None],
        w_query.T,
        w_key.T,
        w_value.T,
        w_output_gate.T,
        w_decay.T,
        w_beta.T,
        head_gain[None],
        head_rates,
        owner,
        state[:, 0],
    )
    heads = exchanged(spread, TP)
    residual, outgoing, slots = local_call(
        functools.partial(mix_kernel, expert_total),
        [(wide, BF16), ((slot_count, width), BF16), ((top_count, seqs), jnp.int32)],
        [],
        1 << 28,
        heads,
        w_mix_out,
        tokens,
        expert_ids.T,
    )
    along_z = exchanged(outgoing.reshape(planes, cores * capacity, width), "z")
    (spread_rows,) = local_call(
        spread_kernel, [((cores, tp_size, count, width), BF16)], [], 1 << 28, along_z
    )
    arrived = exchanged(spread_rows.reshape(cores * tp_size, count, width), PLANE)
    parts, state_out = local_call(
        expert_kernel,
        [((cores, tp_size, count, width), BF16), (new_state.shape, F32)],
        [pltpu.VMEM((cores * count, model_width), BF16), pltpu.SemaphoreType.DMA],
        1 << 30,
        arrived.reshape(cores, tp_size, count, width),
        ffn_gain[None],
        w_gate[0],
        w_up[0],
        w_down[0],
        new_state,
        far_outs=1,
    )
    parts = exchanged(parts.reshape(cores * tp_size, count, width), PLANE)
    (back,) = local_call(
        functools.partial(total_kernel, planes),
        [((planes, cores * capacity, width), BF16)],
        [],
        1 << 28,
        parts.reshape(cores, tp_size, count, width),
    )
    returned = exchanged(back, "z").reshape(expert_total * capacity, width)
    (layer_out,) = local_call(
        combine_kernel, [(wide, BF16)], [], 1 << 26, returned, slots, expert_weights.T, residual
    )
    return (layer_out, state_out[:, None])


def solution(mesh):
    axes = Mesh(mesh.devices.reshape(16, 2, 4, 4), ("z", "c", "y", "x"))
    ep = ("z", "c")
    in_specs = (
        P(ep, TP),
        P(ep, TP, None, None),
        P(),
        P(),
        P(None, TP),
        P(None, TP),
        P(None, TP),
        P(None, TP),
        P(),
        P(),
        P(TP),
        P(TP),
        P(),
        P(None, TP),
        P(ep, None),
        P(ep, None),
        P(ep, None, TP),
        P(ep, None, TP),
        P(ep, TP, None),
    )
    out_specs = (P(ep, TP), P(ep, TP, None, None))
    return jax.shard_map(shards, mesh=axes, in_specs=in_specs, out_specs=out_specs, check_vma=False)
```
